256 devices in a mesh: ep: 32 (over z, x), tp: 8 (over y, core).
Axes of the slice: x: 4, y: 4, z: 8, core: 2. Of those that a mesh axis runs over, the one named last changes fastest.
Arguments:
- tokens: bfloat16 [512, 2048], P('ep'), may hold values from -6 to 6
- attn_gain: float32 [2048], replicated, may hold values from 0.1 to 1.9
- w_query: bfloat16 [2048, 1024], P(None, 'tp'), may hold values from -0.125 to 0.125
- stick_bias: float32 [16], P('tp'), may hold values from -8.5 to -2.5
- kv_cache: bfloat16 [512, 8, 1024, 128], P('ep', 'tp'), may hold values from -6 to 6
- lengths: int32 [512], P('ep'), may hold values from 1 to 1024, as said below
- head_gain: float32 [1024], P('tp'), may hold values from 0.1 to 1.9
- w_attn_out: bfloat16 [1024, 2048], P('tp'), may hold values from -0.1875 to 0.1875
- ffn_gain: float32 [2048], replicated, may hold values from 0.1 to 1.9
- route_expert: int32 [512, 2], P('ep'), may hold values from 0 to 31, as said below
- route_weight: bfloat16 [512, 2], P('ep'), may hold values from 0.049804688 to 1
- w_exp_gate: bfloat16 [32, 2048, 2048], P('ep', None, 'tp'), may hold values from -0.125 to 0.125
- w_exp_up: bfloat16 [32, 2048, 2048], P('ep', None, 'tp'), may hold values from -0.125 to 0.125
- w_exp_down: bfloat16 [32, 2048, 2048], P('ep', 'tp'), may hold values from -0.125 to 0.125
- branch_gate: bfloat16 [2048], replicated, may hold values from -0.125 to 0.125
- w_dense_gate: bfloat16 [8192, 2048], P(('ep', 'tp')), may hold values from -0.125 to 0.125
- w_dense_up: bfloat16 [8192, 2048], P(('ep', 'tp')), may hold values from -0.125 to 0.125
- w_dense_down: bfloat16 [8192, 2048], P(('ep', 'tp')), may hold values from -0.25 to 0.25
Outputs:
- mixed: bfloat16 [512, 2048], P('ep', 'tp')
The draws below stay inside these ranges and needn't reach their ends.
Inputs may be any that keep to these rules, and one draw needn't show every extreme that they name: `route_expert`: each row names 2 different experts of one group (expert x lies in group x // 8). The rows of one index of ep name no expert more than 2 times; one group, the same for every index of ep, has each of its experts named exactly 2 times by the rows of every index of ep. `lengths`: some sequence has length 1024.
All inputs are finite; a program needn't handle non-finite values.
Results may differ from the reference program's by a relative error of at most 0.0076.
Values may be sent and summed in bfloat16 or wider, within the bound.
No kernel may reach another device: no remote copies, remote signals or barrier semaphores. Data moves between devices by JAX's collectives and lax.ppermute only.
A program may use at most 64 MiB of HBM per device.

```python
import math
import jax
import jax.numpy as jnp
from jax import lax

D = 2048
HEADS = 16
HEAD = 64
KV_HEADS = 8
CACHE = 1024
SEQ_DEV = 16
GROUPS = 4
EPG = 8
TOPK = 2
EXP_FF = 2048
DENSE_FF = 8192
EXPERTS = 32
CAP = 2
SEQS = 512
N_EP = 32


def draw_stick_bias(key, part):
    return jax.random.uniform(key, (HEADS,), jnp.float32, -8.0, -2.5)


def draw_lengths(key, part):
    base_key = jax.random.fold_in(key, 5)
    key_shift, key_length, key_row = jax.random.split(base_key, 3)
    block_count = SEQS // SEQ_DEV
    shift_exp = jax.random.randint(key_shift, (block_count, 1), 0, 4)
    block_top = CACHE // jnp.power(2, shift_exp)
    drawn = jax.random.randint(key_length, (block_count, SEQ_DEV), 1, block_top + 1).reshape(SEQS)
    full_row = jax.random.randint(key_row, (), 0, SEQS)
    return jnp.where(jnp.arange(SEQS) == full_row, CACHE, drawn).astype(jnp.int32)


def draw_route_expert(key, part):
    base_key = jax.random.fold_in(key, 11)
    key_group, key_blocks = jax.random.split(base_key)
    most_rows = EPG * CAP // TOPK
    spare_slots = (GROUPS - 1) * most_rows
    full_group = jax.random.randint(key_group, (), 0, GROUPS)
    block_keys = jax.random.split(key_blocks, SEQS // SEQ_DEV)

    def one_block(block_key):
        key_order, key_slots, key_inner = jax.random.split(block_key, 3)
        order = jax.random.permutation(key_order, SEQ_DEV)
        slots = jax.random.permutation(key_slots, spare_slots)
        place = jnp.arange(SEQ_DEV)
        spare = jnp.take(slots, jnp.clip(place - most_rows, 0, spare_slots - 1))
        group_at = jnp.where(place < most_rows, full_group, (full_group + 1 + spare // most_rows) % GROUPS)
        group_of = jnp.zeros((SEQ_DEV,), jnp.int32).at[order].set(group_at.astype(jnp.int32))
        member = (group_of[:, None] == jnp.arange(GROUPS)[None, :]).astype(jnp.int32)
        slot_rank = jnp.sum(member * (jnp.cumsum(member, axis=0) - 1), axis=1)
        inner_scores = jax.random.randint(key_inner, (GROUPS, EPG), 0, 1 << 20) * EPG + jnp.arange(EPG)[None, :]
        inner_order = jnp.argsort(inner_scores, axis=1)
        pick = (TOPK * slot_rank[:, None] + jnp.arange(TOPK)[None, :]) % EPG
        inner = inner_order[group_of[:, None], pick]
        return group_of[:, None] * EPG + inner
    routes = jax.vmap(one_block)(block_keys)
    return routes.reshape(SEQS, TOPK).astype(jnp.int32)


def raised(values, rng, source, target, parts, factor):
    def block_of(axis_at):
        return (jnp.arange(values.shape[axis_at]) // (values.shape[axis_at] // parts)).reshape((-1,) + (1,) * (values.ndim - 1 - axis_at))

    one_side = jax.random.permutation(rng, parts)[block_of(target)]
    other_side = (block_of(target) + parts // 2) % parts
    return jnp.where((block_of(source) == one_side) | (block_of(source) == other_side), factor * values, values)


def block_scale(own_key, extent, pieces, least, top_value):
    level, own = 1.0, jax.random.fold_in(own_key, 6)
    for dim, shards_of in pieces:
        draws = jnp.exp(jax.random.uniform(jax.random.fold_in(own, dim), (shards_of,), jnp.float32, least / len(pieces), top_value / len(pieces)))
        level = level * jnp.repeat(draws, extent[dim] // shards_of).reshape([-1 if axis == dim else 1 for axis in range(len(extent))])
    return level


def scatter_about(stream_key, extent, scale, bound, cuts=(), kind=jnp.bfloat16):
    factor_of = block_scale(stream_key, extent, cuts, -0.22, 0.18) if cuts else 1.0
    values = jax.random.normal(stream_key, extent, jnp.float32) * scale * factor_of
    return jnp.minimum(jnp.maximum(values, -bound), bound).astype(kind)


def bell_draw_with(own_key, shape, scale, limit, pieces, heavy, kind=jnp.bfloat16):
    values = scale * jax.random.normal(own_key, shape, jnp.float32)
    if pieces:
        values = values * block_scale(own_key, shape, pieces, -0.22, 0.18)
    return jnp.clip(raised(values, jax.random.fold_in(own_key, 3), *heavy), -limit, limit).astype(kind)


def setup_inputs(seed: int = 0) -> dict:
    key_of = jax.random.split(jax.random.key(seed), 19)
    return {
        "tokens": scatter_about(key_of[0], (SEQS, D), 1.0, 6.0, ((0, 32),)),
        "attn_gain": jnp.clip(1.0 + 0.18 * jax.random.normal(key_of[1], (D,), jnp.float32), 0.1, 1.9),
        "w_query": scatter_about(key_of[2], (D, HEADS * HEAD), D ** -0.5, 0.125, ((1, 8),)),
        "stick_bias": draw_stick_bias(jax.random.fold_in(key_of[18], 71), 0),
        "kv_cache": scatter_about(key_of[4], (SEQS, KV_HEADS, CACHE, 2 * HEAD), 1.0, 6.0, ((0, 32), (1, 8))),
        "lengths": draw_lengths(jax.random.fold_in(key_of[18], 71), 0),
        "head_gain": jnp.clip(1.0 + 0.18 * jax.random.normal(key_of[6], (HEADS * HEAD,), jnp.float32), 0.1, 1.9),
        "w_attn_out": scatter_about(key_of[7], (HEADS * HEAD, D), (HEADS * HEAD) ** -0.5, 0.1875, ((0, 8),)),
        "ffn_gain": jnp.clip(1.0 + 0.18 * jax.random.normal(key_of[8], (D,), jnp.float32), 0.1, 1.9),
        "route_expert": draw_route_expert(jax.random.fold_in(key_of[18], 71), 0),
        "route_weight": jnp.clip(jnp.exp(math.log(1.0) - 2.9996462 * jax.random.uniform(key_of[10], (SEQS, TOPK), jnp.float32) ** block_scale(key_of[10], (SEQS, TOPK), ((0, 32),), -0.2, 0.2)), 0.049804688, 1.0).astype(jnp.bfloat16),
        "w_exp_gate": scatter_about(key_of[11], (EXPERTS, D, EXP_FF), D ** -0.5, 0.125, ((0, 32), (2, 8))),
        "w_exp_up": scatter_about(key_of[12], (EXPERTS, D, EXP_FF), D ** -0.5, 0.125, ((0, 32), (2, 8))),
        "w_exp_down": scatter_about(key_of[13], (EXPERTS, EXP_FF, D), EXP_FF ** -0.5, 0.125, ((0, 32), (1, 8))),
        "branch_gate": scatter_about(key_of[14], (D,), D ** -0.5, 0.125),
        "w_dense_gate": scatter_about(key_of[15], (DENSE_FF, D), D ** -0.5, 0.125, ((0, 256),)),
        "w_dense_up": scatter_about(key_of[16], (DENSE_FF, D), D ** -0.5, 0.125, ((0, 256),)),
        "w_dense_down": bell_draw_with(key_of[17], (DENSE_FF, D), DENSE_FF ** -0.5, 0.25, ((0, 256),), (0, 1, 256, 6.0)),
    }


epsilon = 1e-06
highest = lax.Precision.HIGHEST

def stored(values):
    return lax.optimization_barrier(values.astype(jnp.bfloat16))

def rms_scale(matrix, gain):
    wide = matrix.astype(jnp.float32)
    return wide * lax.rsqrt(lax.optimization_barrier(jnp.mean(wide * wide, axis=-1, keepdims=True)) + epsilon) * gain

def reference(tokens, attn_gain, w_query, stick_bias, kv_cache, lengths, head_gain, w_attn_out, ffn_gain, route_expert, route_weight, w_exp_gate, w_exp_up, w_exp_down, branch_gate, w_dense_gate, w_dense_up, w_dense_down):
    single = jnp.float32
    group_size = HEADS // KV_HEADS
    normed = stored(rms_scale(tokens, attn_gain))
    query_rows = stored(jnp.dot(normed, w_query, preferred_element_type=single))
    query_rows = query_rows.reshape(N_EP, SEQ_DEV, KV_HEADS, group_size, HEAD)
    cache_blocks = kv_cache.reshape(N_EP, SEQ_DEV, KV_HEADS, CACHE, 2 * HEAD)
    length_blocks = lengths.reshape(N_EP, SEQ_DEV)
    bias_grid = stick_bias.reshape(KV_HEADS, group_size)
    gain_grid = head_gain.reshape(KV_HEADS, group_size, HEAD)

    def attend(item_block):
        query_block, cache_block, length_block = item_block
        key_cols = cache_block[..., :HEAD].astype(single)
        value_cols = cache_block[..., HEAD:].astype(single)
        scores = jnp.einsum('shge,shke->shgk', query_block.astype(single), key_cols, precision=highest)
        scores = scores / math.sqrt(HEAD) + bias_grid[None, :, :, None]
        position = lax.broadcasted_iota(jnp.int32, scores.shape, 3)
        valid_keys = position < length_block[:, None, None, None]
        log_keep = jnp.where(valid_keys, -jax.nn.softplus(scores), 0.0)
        later_sum = lax.cumsum(log_keep, axis=3, reverse=True) - log_keep
        weights = jnp.where(valid_keys, jnp.exp(jax.nn.log_sigmoid(scores) + later_sum), 0.0)
        weights = stored(weights).astype(single)
        head_out = jnp.einsum('shgk,shke->shge', weights, value_cols, precision=highest)
        head_out = head_out * lax.rsqrt(lax.optimization_barrier(jnp.mean(head_out * head_out, axis=-1, keepdims=True)) + epsilon) * gain_grid
        return stored(head_out).reshape(SEQ_DEV, HEADS * HEAD)
    head_rows = lax.map(attend, (query_rows, cache_blocks, length_blocks)).reshape(SEQS, HEADS * HEAD)
    residual = tokens.astype(single) + jnp.dot(head_rows, w_attn_out, preferred_element_type=single)
    normed2 = stored(rms_scale(residual, ffn_gain))
    branch_weight = stored(jax.nn.sigmoid(jnp.dot(normed2, branch_gate, preferred_element_type=single)))
    branch_weight = branch_weight.astype(single)

    def expert_step(running, expert_index):
        hit_table = route_expert == expert_index
        row_weight = lax.optimization_barrier(jnp.sum(jnp.where(hit_table, route_weight.astype(single), 0.0), axis=1))
        used_rows = jnp.any(hit_table, axis=1)
        picked = jnp.nonzero(used_rows, size=N_EP * CAP, fill_value=0)[0].astype(jnp.int32)
        live_rows = jnp.arange(N_EP * CAP, dtype=jnp.int32) < jnp.sum(used_rows.astype(jnp.int32))
        chosen = jnp.take(normed2, picked, axis=0)
        gate_pre = jnp.dot(chosen, lax.dynamic_index_in_dim(w_exp_gate, expert_index, 0, False), preferred_element_type=single)
        up_pre = jnp.dot(chosen, lax.dynamic_index_in_dim(w_exp_up, expert_index, 0, False), preferred_element_type=single)
        hidden = (jax.nn.silu(gate_pre) * up_pre).astype(jnp.bfloat16)
        expert_out = jnp.dot(hidden, lax.dynamic_index_in_dim(w_exp_down, expert_index, 0, False), preferred_element_type=single)
        addend = jnp.where(live_rows[:, None], jnp.take(row_weight, picked)[:, None] * expert_out, 0.0)
        return (running.at[picked].add(addend), None)
    routed, _ = lax.scan(expert_step, jnp.zeros((SEQS, D), single), jnp.arange(EXPERTS, dtype=jnp.int32))
    contract = (((1,), (1,)), ((), ()))
    dense_gate_pre = lax.dot_general(normed2, w_dense_gate, contract, preferred_element_type=single)
    dense_up_pre = lax.dot_general(normed2, w_dense_up, contract, preferred_element_type=single)
    dense_hidden = (jax.nn.silu(dense_gate_pre) * dense_up_pre).astype(jnp.bfloat16)
    dense_out = jnp.dot(dense_hidden, w_dense_down, preferred_element_type=single)
    return (residual + routed + branch_weight[:, None] * dense_out).astype(jnp.bfloat16)
```

```python
import jax
import jax.numpy as jnp
from jax import lax
from jax.experimental import pallas as pl
from jax.experimental.pallas import tpu as pltpu
from jax.sharding import PartitionSpec as P

HEADS = 16
HEAD = 64
KV_HEADS = 8
EXPERTS = 32
CAP = 2
CACHE = 1024
WIDTH = 2048
ROWS = 16
LANES = 128
HALF = 8
epsilon = 1e-06
NT = (((1,), (1,)), ((), ()))


def attention_kernel(
    len_ref, bias_ref, tok_ref, gain_ref, hgain_ref, wq_hbm, kv_hbm, wo_hbm,
    out_ref, wq_v, kv_v, wo_v, q_sem, kv_sem, o_sem,
):
    copy_q = pltpu.make_async_copy(wq_hbm, wq_v, q_sem)
    copy_q.start()
    copies = []
    for s in range(ROWS):
        half, j = divmod(s, HALF)
        copy = pltpu.make_async_copy(
            kv_hbm.at[s, 0], kv_v.at[half, :, pl.ds(j * LANES, LANES)], kv_sem.at[s]
        )
        copy.start()
        copies.append(copy)
    copy_o = pltpu.make_async_copy(wo_hbm, wo_v, o_sem)
    copy_o.start()

    wide = tok_ref[...].astype(jnp.float32)
    scale = lax.rsqrt(jnp.mean(wide * wide, axis=-1, keepdims=True) + epsilon)
    normed = (wide * scale * gain_ref[...]).astype(jnp.bfloat16)
    copy_q.wait()
    query = jnp.dot(normed, wq_v[...], preferred_element_type=jnp.float32)
    query = query.astype(jnp.bfloat16).astype(jnp.float32)

    lane8 = lax.broadcasted_iota(jnp.int32, (HALF, LANES), 1)
    row8 = lax.broadcasted_iota(jnp.int32, (HALF, LANES), 0)
    lane16 = lax.broadcasted_iota(jnp.int32, (2 * HALF, LANES), 1)
    row16 = lax.broadcasted_iota(jnp.int32, (2 * HALF, LANES), 0)
    tri_row = lax.broadcasted_iota(jnp.int32, (LANES, 2 * LANES), 0)
    tri_col = lax.broadcasted_iota(jnp.int32, (LANES, 2 * LANES), 1)
    tri = ((tri_row >= tri_col) | (tri_col >= LANES)).astype(jnp.bfloat16)
    position = lax.broadcasted_iota(jnp.int32, (2 * HALF, CACHE), 1)
    bias = jnp.where(row16[:, :1] < HALF, bias_ref[0], bias_ref[1])
    hgain = hgain_ref[...]
    gain_rows = jnp.where(row16 < HALF, pltpu.roll(hgain, HEAD, 1), hgain)
    chunks = CACHE // LANES

    heads = []
    for half in range(2):
        part = query[half * HALF : (half + 1) * HALF]
        first = jnp.where(lane8 < HEAD, part, 0.0)
        second = jnp.where(lane8 < HEAD, pltpu.roll(part, HEAD, 1), 0.0)
        blocks = [
            jnp.concatenate(
                [jnp.where(row8 == j, first, 0.0), jnp.where(row8 == j, second, 0.0)], axis=0
            )
            for j in range(HALF)
        ]
        lhs = jnp.concatenate(blocks, axis=1).astype(jnp.bfloat16)
        length = jnp.full((2 * HALF, 1), len_ref[half * HALF], jnp.int32)
        for j in range(1, HALF):
            length = jnp.where(row16[:, :1] % HALF == j, len_ref[half * HALF + j], length)
        valid = position < length
        for j in range(HALF):
            copies[half * HALF + j].wait()
        scores = lax.dot_general(lhs, kv_v[half], NT, preferred_element_type=jnp.float32)
        scores = scores * 0.125 + bias
        soft = jnp.maximum(scores, 0.0) + jnp.log1p(jnp.exp(-jnp.abs(scores)))
        soft = jnp.where(valid, soft, 0.0)
        stacked = jnp.concatenate(
            [soft[:, c * LANES : (c + 1) * LANES] for c in range(chunks)], axis=0
        )
        high = stacked.astype(jnp.bfloat16)
        rest = stacked - high.astype(jnp.float32)
        middle = rest.astype(jnp.bfloat16)
        low = (rest - middle.astype(jnp.float32)).astype(jnp.bfloat16)
        sums = jnp.dot(high, tri, preferred_element_type=jnp.float32)
        sums = sums + jnp.dot(middle, tri, preferred_element_type=jnp.float32)
        sums = sums + jnp.dot(low, tri, preferred_element_type=jnp.float32)
        pieces = [None] * chunks
        carry = jnp.zeros((2 * HALF, LANES), jnp.float32)
        for c in reversed(range(chunks)):
            rows = sums[c * 2 * HALF : (c + 1) * 2 * HALF]
            pieces[c] = rows[:, :LANES] + carry
            carry = carry + rows[:, LANES:]
        later = jnp.concatenate(pieces, axis=1)
        weights = jnp.where(valid, jnp.exp(scores - later), 0.0).astype(jnp.bfloat16)
        mixed = jnp.dot(weights, kv_v[half], preferred_element_type=jnp.float32)
        own = jnp.zeros((2 * HALF, LANES), jnp.float32)
        for j in range(HALF):
            own = jnp.where(row16 % HALF == j, mixed[:, j * LANES : (j + 1) * LANES], own)
        square = jnp.where(lane16 >= HEAD, own * own, 0.0)
        mean = jnp.sum(square, axis=-1, keepdims=True) * (1.0 / HEAD)
        own = own * lax.rsqrt(mean + epsilon) * gain_rows
        heads.append(
            jnp.where(lane8 < HEAD, pltpu.roll(own[:HALF], HEAD, 1), own[HALF:])
        )
    head_rows = jnp.concatenate(heads, axis=0).astype(jnp.bfloat16)
    copy_o.wait()
    share = jnp.dot(head_rows, wo_v[...], preferred_element_type=jnp.float32)
    share = share.astype(jnp.bfloat16)
    for i in range(8):
        out_ref[i] = share


def attention(tokens, attn_gain, w_query, stick_bias, kv_cache, lengths, head_gain, w_attn_out):
    vmem = pl.BlockSpec(memory_space=pltpu.VMEM)
    smem = pl.BlockSpec(memory_space=pltpu.SMEM)
    anywhere = pl.BlockSpec(memory_space=pl.ANY)
    return pl.pallas_call(
        attention_kernel,
        out_shape=jax.ShapeDtypeStruct((8, ROWS, WIDTH), jnp.bfloat16),
        in_specs=[smem, smem, vmem, vmem, vmem, anywhere, anywhere, anywhere],
        out_specs=vmem,
        scratch_shapes=[
            pltpu.VMEM((WIDTH, LANES), jnp.bfloat16),
            pltpu.VMEM((2, CACHE, HALF * LANES), jnp.bfloat16),
            pltpu.VMEM((LANES, WIDTH), jnp.bfloat16),
            pltpu.SemaphoreType.DMA,
            pltpu.SemaphoreType.DMA((ROWS,)),
            pltpu.SemaphoreType.DMA,
        ],
        cost_estimate=pl.CostEstimate(
            flops=400_000_000, bytes_accessed=6_000_000, transcendentals=200_000
        ),
    )(
        lengths, stick_bias, tokens, attn_gain.reshape(1, -1), head_gain.reshape(1, -1),
        w_query, kv_cache, w_attn_out,
    )


def slot_table(routes):
    ids = jnp.arange(EXPERTS, dtype=jnp.int32)
    hits = (routes[..., None] == ids).astype(jnp.int32)
    per_row = jnp.sum(hits, axis=1)
    before = jnp.arange(ROWS)[:, None] > jnp.arange(ROWS)[None, :]
    earlier = jnp.sum(jnp.where(before[:, :, None], per_row[None], 0), axis=1)
    rank = jnp.sum(hits * earlier[:, None, :], axis=-1)
    slot = jnp.arange(CAP, dtype=jnp.int32)
    return (routes[:, :, None, None] == ids[:, None]) & (rank[:, :, None, None] == slot)


def gated(rows, gate, up, down, dims):
    a = lax.dot_general(rows, gate, dims, preferred_element_type=jnp.float32)
    b = lax.dot_general(rows, up, dims, preferred_element_type=jnp.float32)
    hidden = (jax.nn.silu(a) * b).astype(jnp.bfloat16)
    return jnp.dot(hidden, down, preferred_element_type=jnp.float32).astype(jnp.bfloat16)


def shards(
    tokens, attn_gain, w_query, stick_bias, kv_cache, lengths, head_gain, w_attn_out, ffn_gain,
    route_expert, route_weight, w_exp_gate, w_exp_up, w_exp_down, branch_gate,
    w_dense_gate, w_dense_up, w_dense_down,
):
    single = jnp.float32
    t = lax.axis_index("tp")
    core = t % 2
    copies = attention(
        tokens, attn_gain, w_query, stick_bias, kv_cache, lengths, head_gain, w_attn_out
    )
    copies, route_expert, w_dense_gate, w_dense_up, w_dense_down = lax.optimization_barrier(
        (copies, route_expert, w_dense_gate, w_dense_up, w_dense_down)
    )
    shares = lax.all_to_all(copies, "tp", 0, 0, tiled=True)

    own = jnp.stack([w_dense_gate, w_dense_up, w_dense_down])
    groups = [[z * 4 + x for x in range(4)] for z in range(8)]
    four = lax.all_to_all(
        jnp.broadcast_to(own[None], (4, *own.shape)), "ep", 0, 0, tiled=True,
        axis_index_groups=groups,
    )
    other = lax.ppermute(four, "tp", [(i, i ^ 1) for i in range(8)])

    table = slot_table(route_expert)
    taken = jnp.any(table, axis=1)
    expert_dest = jnp.moveaxis(taken, 0, -1)
    quarter = 4 * (jnp.arange(32) % 4)[:, None] + 2 * core + jnp.arange(2)
    dense_dest = quarter[..., None] == jnp.arange(ROWS)
    picks = jnp.concatenate([expert_dest, dense_dest], axis=1)

    residual = tokens.astype(single) + jnp.sum(shares.astype(single), axis=0)
    scale = lax.rsqrt(jnp.mean(residual * residual, axis=-1, keepdims=True) + epsilon)
    normed = (residual * scale * ffn_gain).astype(jnp.bfloat16)
    branch = jax.nn.sigmoid(jnp.dot(normed, branch_gate, preferred_element_type=single))
    branch = branch.astype(jnp.bfloat16)
    residual_cols = lax.dynamic_slice_in_dim(residual, t * 256, 256, 1)

    send = jnp.einsum(
        "cks,sd->ckd", picks.astype(jnp.bfloat16), normed, preferred_element_type=single
    ).astype(jnp.bfloat16)
    got = lax.all_to_all(send, "ep", 0, 0, tiled=True)

    expert_rows = got[:, :2].reshape(64, WIDTH)
    dense_rows = got[:, 2:].reshape(64, WIDTH)
    expert_out = gated(
        expert_rows, w_exp_gate[0], w_exp_up[0], w_exp_down[0], (((1,), (0,)), ((), ()))
    )
    weights = jnp.concatenate([four, other], axis=0)
    gate_all = weights[:, 0].reshape(256, WIDTH)
    up_all = weights[:, 1].reshape(256, WIDTH)
    down_all = weights[:, 2].reshape(256, WIDTH)
    dense_out = gated(dense_rows, gate_all, up_all, down_all, NT)
    back = jnp.concatenate(
        [expert_out.reshape(32, 2, WIDTH), dense_out.reshape(32, 2, WIDTH)], axis=1
    )
    returned = lax.all_to_all(back, "ep", 0, 0, tiled=True).reshape(128, WIDTH)

    weight = jnp.sum(
        jnp.where(table, route_weight[:, :, None, None].astype(single), 0.0), axis=1
    ).astype(jnp.bfloat16)
    dense_weight = jnp.where(
        jnp.moveaxis(dense_dest, -1, 0), branch[:, None, None], jnp.bfloat16(0)
    )
    mix = jnp.concatenate([weight, dense_weight], axis=2).reshape(ROWS, 128)
    partial = jnp.dot(mix, returned, preferred_element_type=single).astype(jnp.bfloat16)
    partial = jnp.moveaxis(partial.reshape(ROWS, 8, 256), 1, 0)
    columns = lax.all_to_all(partial, "tp", 0, 0, tiled=True)
    total = jnp.sum(columns.astype(single), axis=0)
    return (residual_cols + total).astype(jnp.bfloat16)


def solution(mesh):
    return jax.shard_map(
        shards,
        mesh=mesh,
        in_specs=(
            P("ep", None), P(), P(None, "tp"), P("tp"), P("ep", "tp", None, None), P("ep"),
            P("tp"), P("tp", None), P(), P("ep", None), P("ep", None), P("ep", None, "tp"),
            P("ep", None, "tp"), P("ep", "tp", None), P(), P(("ep", "tp"), None),
            P(("ep", "tp"), None), P(("ep", "tp"), None),
        ),
        out_specs=P("ep", "tp"),
        check_vma=False,
    )
```

```python
import jax
import jax.numpy as jnp
from jax import lax
from jax.experimental import pallas as pl
from jax.experimental.pallas import tpu as pltpu
from jax.sharding import PartitionSpec as P


HEAD = 64
EXPERTS = 32
CAP = 2
CACHE = 1024
WIDTH = 2048
ROWS = 16
LANES = 128
HALF = 8
MIB = 1 << 20
MESSAGES = 512
PART = 512
epsilon = 1e-06
NT = (((1,), (1,)), ((), ()))


def attention_kernel(
    len_ref, bias_ref, tok_ref, gain_ref, hgain_ref, wq_hbm, kv_hbm, wo_hbm,
    out_ref, wq_v, kv_v, wo_v, q_sem, kv_sem, o_sem,
):
    copy_q = pltpu.make_async_copy(wq_hbm, wq_v, q_sem)
    copy_q.start()
    copies = []
    for s in range(ROWS):
        half, j = divmod(s, HALF)
        copy = pltpu.make_async_copy(
            kv_hbm.at[s, 0], kv_v.at[half, :, pl.ds(j * LANES, LANES)], kv_sem.at[s]
        )
        copy.start()
        copies.append(copy)
    copy_o = pltpu.make_async_copy(wo_hbm, wo_v, o_sem)
    copy_o.start()

    wide = tok_ref[...].astype(jnp.float32)
    scale = lax.rsqrt(jnp.mean(wide * wide, axis=-1, keepdims=True) + epsilon)
    normed = (wide * scale * gain_ref[...]).astype(jnp.bfloat16)
    copy_q.wait()
    query = jnp.dot(normed, wq_v[...], preferred_element_type=jnp.float32)
    query = query.astype(jnp.bfloat16).astype(jnp.float32)

    lane8 = lax.broadcasted_iota(jnp.int32, (HALF, LANES), 1)
    row8 = lax.broadcasted_iota(jnp.int32, (HALF, LANES), 0)
    lane16 = lax.broadcasted_iota(jnp.int32, (2 * HALF, LANES), 1)
    row16 = lax.broadcasted_iota(jnp.int32, (2 * HALF, LANES), 0)
    tri_row = lax.broadcasted_iota(jnp.int32, (LANES, 2 * LANES), 0)
    tri_col = lax.broadcasted_iota(jnp.int32, (LANES, 2 * LANES), 1)
    tri = ((tri_row >= tri_col) | (tri_col >= LANES)).astype(jnp.bfloat16)
    position = lax.broadcasted_iota(jnp.int32, (2 * HALF, CACHE), 1)
    bias = jnp.where(row16[:, :1] < HALF, bias_ref[0], bias_ref[1])
    hgain = hgain_ref[...]
    gain_rows = jnp.where(row16 < HALF, pltpu.roll(hgain, HEAD, 1), hgain)
    chunks = CACHE // LANES

    heads = []
    for half in range(2):
        part = query[half * HALF : (half + 1) * HALF]
        first = jnp.where(lane8 < HEAD, part, 0.0)
        second = jnp.where(lane8 < HEAD, pltpu.roll(part, HEAD, 1), 0.0)
        blocks = [
            jnp.concatenate(
                [jnp.where(row8 == j, first, 0.0), jnp.where(row8 == j, second, 0.0)], axis=0
            )
            for j in range(HALF)
        ]
        lhs = jnp.concatenate(blocks, axis=1).astype(jnp.bfloat16)
        length = jnp.full((2 * HALF, 1), len_ref[half * HALF], jnp.int32)
        for j in range(1, HALF):
            length = jnp.where(row16[:, :1] % HALF == j, len_ref[half * HALF + j], length)
        valid = position < length
        for j in range(HALF):
            copies[half * HALF + j].wait()
        scores = lax.dot_general(lhs, kv_v[half], NT, preferred_element_type=jnp.float32)
        scores = scores * 0.125 + bias
        soft = jnp.maximum(scores, 0.0) + jnp.log1p(jnp.exp(-jnp.abs(scores)))
        soft = jnp.where(valid, soft, 0.0)
        stacked = jnp.concatenate(
            [soft[:, c * LANES : (c + 1) * LANES] for c in range(chunks)], axis=0
        )
        high = stacked.astype(jnp.bfloat16)
        rest = stacked - high.astype(jnp.float32)
        middle = rest.astype(jnp.bfloat16)
        low = (rest - middle.astype(jnp.float32)).astype(jnp.bfloat16)
        sums = jnp.dot(high, tri, preferred_element_type=jnp.float32)
        sums = sums + jnp.dot(middle, tri, preferred_element_type=jnp.float32)
        sums = sums + jnp.dot(low, tri, preferred_element_type=jnp.float32)
        pieces = [None] * chunks
        carry = jnp.zeros((2 * HALF, LANES), jnp.float32)
        for c in reversed(range(chunks)):
            rows = sums[c * 2 * HALF : (c + 1) * 2 * HALF]
            pieces[c] = rows[:, :LANES] + carry
            carry = carry + rows[:, LANES:]
        later = jnp.concatenate(pieces, axis=1)
        weights = jnp.where(valid, jnp.exp(scores - later), 0.0).astype(jnp.bfloat16)
        mixed = jnp.dot(weights, kv_v[half], preferred_element_type=jnp.float32)
        own = jnp.zeros((2 * HALF, LANES), jnp.float32)
        for j in range(HALF):
            own = jnp.where(row16 % HALF == j, mixed[:, j * LANES : (j + 1) * LANES], own)
        square = jnp.where(lane16 >= HEAD, own * own, 0.0)
        mean = jnp.sum(square, axis=-1, keepdims=True) * (1.0 / HEAD)
        own = own * lax.rsqrt(mean + epsilon) * gain_rows
        heads.append(
            jnp.where(lane8 < HEAD, pltpu.roll(own[:HALF], HEAD, 1), own[HALF:])
        )
    head_rows = jnp.concatenate(heads, axis=0).astype(jnp.bfloat16)
    copy_o.wait()
    share = jnp.dot(head_rows, wo_v[...], preferred_element_type=jnp.float32)
    share = share.astype(jnp.bfloat16)
    for i in range(8):
        out_ref[i] = share


def attention(tokens, attn_gain, w_query, stick_bias, kv_cache, lengths, head_gain, w_attn_out):
    vmem = pl.BlockSpec(memory_space=pltpu.VMEM)
    smem = pl.BlockSpec(memory_space=pltpu.SMEM)
    anywhere = pl.BlockSpec(memory_space=pltpu.HBM)
    return pl.pallas_call(
        attention_kernel,
        out_shape=jax.ShapeDtypeStruct((8, ROWS, WIDTH), jnp.bfloat16),
        in_specs=[smem, smem, vmem, vmem, vmem, anywhere, anywhere, anywhere],
        out_specs=vmem,
        scratch_shapes=[
            pltpu.VMEM((WIDTH, LANES), jnp.bfloat16),
            pltpu.VMEM((2, CACHE, HALF * LANES), jnp.bfloat16),
            pltpu.VMEM((LANES, WIDTH), jnp.bfloat16),
            pltpu.SemaphoreType.DMA,
            pltpu.SemaphoreType.DMA((ROWS,)),
            pltpu.SemaphoreType.DMA,
        ],
        cost_estimate=pl.CostEstimate(
            flops=400_000_000, bytes_accessed=6_000_000, transcendentals=200_000
        ),
    )(
        lengths, stick_bias, tokens, attn_gain.reshape(1, -1), head_gain.reshape(1, -1),
        w_query, kv_cache, w_attn_out,
    )


def dispatch_kernel(shares_ref, tok_ref, gain_ref, gate_ref, pick_ref, send_ref, res_ref, branch_ref):
    total = tok_ref[...].astype(jnp.float32)
    for i in range(8):
        total = total + shares_ref[i].astype(jnp.float32)
    res_ref[...] = total
    scale = lax.rsqrt(jnp.mean(total * total, axis=-1, keepdims=True) + epsilon)
    normed = (total * scale * gain_ref[...]).astype(jnp.bfloat16)
    logit = jnp.sum(
        normed.astype(jnp.float32) * gate_ref[...].astype(jnp.float32), axis=-1, keepdims=True
    )
    branch_ref[...] = jnp.broadcast_to(1.0 / (1.0 + jnp.exp(-logit)), branch_ref.shape)
    stacked = jnp.concatenate([normed[:, q * PART : (q + 1) * PART] for q in range(4)], axis=0)
    send_ref[...] = jnp.dot(
        pick_ref[...], stacked, preferred_element_type=jnp.float32
    ).astype(jnp.bfloat16)


def dispatch(shares, tokens, ffn_gain, branch_gate, picks):
    vmem = pl.BlockSpec(memory_space=pltpu.VMEM)
    return pl.pallas_call(
        dispatch_kernel,
        out_shape=(
            jax.ShapeDtypeStruct((MESSAGES, PART), jnp.bfloat16),
            jax.ShapeDtypeStruct((ROWS, WIDTH), jnp.float32),
            jax.ShapeDtypeStruct((ROWS, LANES), jnp.float32),
        ),
        in_specs=[vmem] * 5,
        out_specs=(vmem, vmem, vmem),
        compiler_params=pltpu.CompilerParams(vmem_limit_bytes=8 * MIB),
        cost_estimate=pl.CostEstimate(
            flops=40_000_000, bytes_accessed=1_500_000, transcendentals=100
        ),
    )(shares, tokens, ffn_gain.reshape(1, -1), branch_gate.reshape(1, -1), picks)


def feed_kernel(
    got_ref, eg_hbm, eu_hbm, ed_hbm, *rest,
):
    packs = rest[:8]
    out_ref, wide_v, eg_v, eu_v, ed_v, dg_v, du_v, dd_v, e_sem, d_sem = rest[8:]
    expert_copies = [
        pltpu.make_async_copy(src, dst, e_sem.at[k])
        for k, (src, dst) in enumerate(((eg_hbm, eg_v), (eu_hbm, eu_v), (ed_hbm, ed_v)))
    ]
    dense_copies = [
        pltpu.make_async_copy(pack.at[k], dst.at[pl.ds(32 * i, 32), :], d_sem.at[3 * i + k])
        for k, dst in enumerate((dg_v, du_v, dd_v))
        for i, pack in enumerate(packs)
    ]
    for copy in expert_copies + dense_copies:
        copy.start()
    for l in range(4):
        wide_v[l] = got_ref[:, l * LANES : (l + 1) * LANES].astype(jnp.float32)

    def picked(kind, q, slot):
        return pl.ds(kind * 8 + q * 2 + slot, 32, stride=16)

    def unpacked(kind):
        parts = [
            jnp.concatenate([wide_v[l, picked(kind, q, slot), :] for slot in range(2)], axis=0)
            for q in range(4)
            for l in range(4)
        ]
        return jnp.concatenate(parts, axis=1).astype(jnp.bfloat16)

    def packed(kind, value):
        for q in range(4):
            for l in range(4):
                at = q * PART + l * LANES
                for slot in range(2):
                    wide_v[l, picked(kind, q, slot), :] = value[
                        slot * 32 : slot * 32 + 32, at : at + LANES
                    ]

    rows = unpacked(0)
    dense_rows = unpacked(1)
    expert_copies[0].wait()
    a = jnp.dot(rows, eg_v[...], preferred_element_type=jnp.float32)
    expert_copies[1].wait()
    b = jnp.dot(rows, eu_v[...], preferred_element_type=jnp.float32)
    hidden = (a / (1.0 + jnp.exp(-a)) * b).astype(jnp.bfloat16)
    expert_copies[2].wait()
    packed(0, jnp.dot(hidden, ed_v[...], preferred_element_type=jnp.float32))
    for copy in dense_copies:
        copy.wait()
    a = lax.dot_general(dense_rows, dg_v[...], NT, preferred_element_type=jnp.float32)
    b = lax.dot_general(dense_rows, du_v[...], NT, preferred_element_type=jnp.float32)
    hidden = (a / (1.0 + jnp.exp(-a)) * b).astype(jnp.bfloat16)
    packed(1, jnp.dot(hidden, dd_v[...], preferred_element_type=jnp.float32))
    for l in range(4):
        out_ref[:, l * LANES : (l + 1) * LANES] = wide_v[l].astype(jnp.bfloat16)


def feed(got, gate, up, down, packs):
    vmem = pl.BlockSpec(memory_space=pltpu.VMEM)
    hbm = pl.BlockSpec(memory_space=pltpu.HBM)
    return pl.pallas_call(
        feed_kernel,
        out_shape=jax.ShapeDtypeStruct((MESSAGES, PART), jnp.bfloat16),
        in_specs=[vmem] + [hbm] * 11,
        out_specs=vmem,
        scratch_shapes=[
            pltpu.VMEM((4, MESSAGES, LANES), jnp.float32),
            pltpu.VMEM((WIDTH, 256), jnp.bfloat16),
            pltpu.VMEM((WIDTH, 256), jnp.bfloat16),
            pltpu.VMEM((256, WIDTH), jnp.bfloat16),
            pltpu.VMEM((256, WIDTH), jnp.bfloat16),
            pltpu.VMEM((256, WIDTH), jnp.bfloat16),
            pltpu.VMEM((256, WIDTH), jnp.bfloat16),
            pltpu.SemaphoreType.DMA((3,)),
            pltpu.SemaphoreType.DMA((24,)),
        ],
        compiler_params=pltpu.CompilerParams(vmem_limit_bytes=60 * 1024 * 1024 - 640 * 1024),
        cost_estimate=pl.CostEstimate(
            flops=1_000_000_000, bytes_accessed=7_000_000, transcendentals=40_000
        ),
    )(got, gate, up, down, *packs)


def combine_kernel(mix_ref, got_ref, out_ref):
    total = jnp.dot(mix_ref[...], got_ref[...], preferred_element_type=jnp.float32)
    total = total.astype(jnp.bfloat16)
    for t in range(8):
        q, h = divmod(t, 2)
        out_ref[t] = total[q * ROWS : (q + 1) * ROWS, h * 256 : (h + 1) * 256]


def combine(mix, returned):
    vmem = pl.BlockSpec(memory_space=pltpu.VMEM)
    return pl.pallas_call(
        combine_kernel,
        out_shape=jax.ShapeDtypeStruct((8, ROWS, 256), jnp.bfloat16),
        in_specs=[vmem] * 2,
        out_specs=vmem,
        compiler_params=pltpu.CompilerParams(vmem_limit_bytes=4 * MIB),
        cost_estimate=pl.CostEstimate(
            flops=40_000_000, bytes_accessed=600_000, transcendentals=0
        ),
    )(mix, returned)


def slot_table(routes):
    ids = jnp.arange(EXPERTS, dtype=jnp.int32)
    hits = (routes[..., None] == ids).astype(jnp.int32)
    per_row = jnp.sum(hits, axis=1)
    before = jnp.arange(ROWS)[:, None] > jnp.arange(ROWS)[None, :]
    earlier = jnp.sum(jnp.where(before[:, :, None], per_row[None], 0), axis=1)
    rank = jnp.sum(hits * earlier[:, None, :], axis=-1)
    slot = jnp.arange(CAP, dtype=jnp.int32)
    return (routes[:, :, None, None] == ids[:, None]) & (rank[:, :, None, None] == slot)


def layer(
    tokens, attn_gain, w_query, stick_bias, kv_cache, lengths, head_gain, w_attn_out, ffn_gain,
    route_expert, route_weight, w_exp_gate, w_exp_up, w_exp_down, branch_gate,
    w_dense_gate, w_dense_up, w_dense_down,
):
    single, half = jnp.float32, jnp.bfloat16
    t = lax.axis_index("tp")
    core = t % 2
    copies = attention(
        tokens, attn_gain, w_query, stick_bias, kv_cache, lengths, head_gain, w_attn_out
    )
    copies, route_expert, w_dense_gate, w_dense_up, w_dense_down = lax.optimization_barrier(
        (copies, route_expert, w_dense_gate, w_dense_up, w_dense_down)
    )
    shares = lax.all_to_all(copies, "tp", 0, 0, tiled=True)

    own = jnp.stack([w_dense_gate, w_dense_up, w_dense_down])
    packs = [own]
    for m in (1, 4, 5):
        packs.append(lax.ppermute(own, "ep", [(i, i ^ m) for i in range(32)]))
    for k in range(4):
        packs.append(lax.ppermute(packs[k], "tp", [(i, i ^ 1) for i in range(8)]))

    table = slot_table(route_expert)
    taken = jnp.any(table, axis=1)
    dest = jnp.arange(32)
    first = 4 * (2 * (dest // 4 % 2) + dest % 2) + 2 * core
    quarter = first[:, None] + jnp.arange(2)
    expert_dest = jnp.moveaxis(taken, 0, -1)
    dense_dest = quarter[..., None] == jnp.arange(ROWS)
    both = jnp.stack([expert_dest, dense_dest], axis=1)
    eye = jnp.arange(4)[:, None] == jnp.arange(4)
    picks = both[:, :, None, :, None, :] & eye[None, None, :, None, :, None]
    picks = picks.reshape(MESSAGES, 4 * ROWS).astype(half)

    send, residual, branch = dispatch(shares, tokens, ffn_gain, branch_gate, picks)
    got = lax.all_to_all(send.reshape(32, 16, PART), "ep", 0, 0, tiled=True)

    back = feed(
        got.reshape(MESSAGES, PART), w_exp_gate[0], w_exp_up[0], w_exp_down[0], packs
    )
    returned = lax.all_to_all(back.reshape(32, 16, PART), "ep", 0, 0, tiled=True)

    weight = jnp.sum(
        jnp.where(table, route_weight[:, :, None, None].astype(single), 0.0), axis=1
    )
    dense_weight = jnp.where(
        jnp.moveaxis(dense_dest, -1, 0), branch[:, :1, None], 0.0
    )
    mix = jnp.stack([weight, dense_weight], axis=2).astype(half)
    mix = jnp.where(eye[:, None, None, None, :, None], mix[None, :, :, :, None, :], half(0))
    mix = mix.reshape(4 * ROWS, MESSAGES)
    partial = combine(mix, returned.reshape(MESSAGES, PART))
    columns = lax.all_to_all(partial, "tp", 0, 0, tiled=True)
    residual_cols = lax.dynamic_slice_in_dim(residual, t * 256, 256, 1)
    total = jnp.sum(columns.astype(single), axis=0)
    return (residual_cols + total).astype(half)


def solution(mesh):
    return jax.shard_map(
        layer,
        mesh=mesh,
        in_specs=(
            P("ep", None), P(), P(None, "tp"), P("tp"), P("ep", "tp", None, None), P("ep"),
            P("tp"), P("tp", None), P(), P("ep", None), P("ep", None), P("ep", None, "tp"),
            P("ep", None, "tp"), P("ep", "tp", None), P(), P(("ep", "tp"), None),
            P(("ep", "tp"), None), P(("ep", "tp"), None),
        ),
        out_specs=P("ep", "tp"),
        check_vma=False,
    )
```

```python
import jax
import jax.numpy as jnp
from jax import lax
from jax.experimental import pallas as pl
from jax.experimental.pallas import tpu as pltpu
from jax.sharding import PartitionSpec as P


HEAD = 64
CACHE = 1024
WIDTH = 2048
ROWS = 16
LANES = 128
HALF = 8
KIB = 1024
MESSAGES = 512
PART = 512
RETURNED = 2048
epsilon = 1e-06
NT = (((1,), (1,)), ((), ()))
VMEM = pl.BlockSpec(memory_space=pltpu.VMEM)
SMEM = pl.BlockSpec(memory_space=pltpu.SMEM)
HBM = pl.BlockSpec(memory_space=pltpu.HBM)


def columns_of(pair):
    r = lax.broadcasted_iota(jnp.int32, (ROWS, ROWS), 0)
    c = lax.broadcasted_iota(jnp.int32, (ROWS, ROWS), 1)
    pair = pair.astype(jnp.float32)
    return [
        jnp.sum(jnp.where(r == c, pair[k : k + 1], 0.0), axis=-1, keepdims=True) for k in range(2)
    ]


def hits_of(routes, expert, slot):
    first, second = [expert == c.astype(jnp.int32) for c in columns_of(routes)]
    hit = (first | second).astype(jnp.float32).astype(jnp.bfloat16)
    r = lax.broadcasted_iota(jnp.int32, (ROWS, ROWS), 0)
    c = lax.broadcasted_iota(jnp.int32, (ROWS, ROWS), 1)
    before = jnp.dot(
        (c < r).astype(jnp.float32).astype(jnp.bfloat16), hit, preferred_element_type=jnp.float32
    )
    right = before == slot.astype(jnp.float32)
    return first & right, second & right


def quarter_of(device, core, slot):
    return 4 * (2 * ((device >> 2) & 1) + (device & 1)) + 2 * core + slot


def picks_of(routes):
    core = lax.axis_index("tp") % 2
    shape = (ROWS, MESSAGES)
    row = lax.broadcasted_iota(jnp.int32, shape, 0)
    col = lax.broadcasted_iota(jnp.int32, shape, 1)
    device, kind, q, slot = 31 - (col >> 4), (col >> 3) & 1, (col >> 1) & 3, col & 1
    first, second = hits_of(routes, device, slot)
    expert = (first | second) & (kind == 0)
    dense = (row == quarter_of(device, core, slot)) & (kind == 1)
    pick = jnp.where(expert | dense, 1.0, 0.0)
    stacked = jnp.concatenate([jnp.where(q == k, pick, 0.0) for k in range(4)], axis=0)
    return stacked.astype(jnp.bfloat16)


def attention_kernel(
    len_ref, bias_ref, tok_ref, gain_ref, hgain_ref, route_ref, wq_hbm, kv_hbm, wo_hbm,
    out_ref, pick_ref,
    wq_v, kv_v, key_v, value_v, wo_v, q_sem, kv_sem, o_sem,
):
    copy_q = pltpu.make_async_copy(wq_hbm, wq_v, q_sem)
    copy_q.start()
    copies = []
    for s in range(ROWS):
        copy = pltpu.make_async_copy(kv_hbm.at[s, 0], kv_v.at[s], kv_sem.at[s])
        copy.start()
        copies.append(copy)
    copy_o = pltpu.make_async_copy(wo_hbm, wo_v, o_sem)
    copy_o.start()
    wide = tok_ref[...].astype(jnp.float32)
    scale = lax.rsqrt(jnp.mean(wide * wide, axis=-1, keepdims=True) + epsilon)
    normed = (wide * scale * gain_ref[...]).astype(jnp.bfloat16)
    normed = jnp.concatenate([normed[:, : WIDTH // 2], normed[:, WIDTH // 2 :]], axis=0)
    pick_ref[...] = picks_of(route_ref[...])

    lane = lax.broadcasted_iota(jnp.int32, (HALF, LANES), 1)
    row = lax.broadcasted_iota(jnp.int32, (HALF, LANES), 0)
    tri_row = lax.broadcasted_iota(jnp.int32, (LANES, 2 * LANES), 0)
    tri_col = lax.broadcasted_iota(jnp.int32, (LANES, 2 * LANES), 1)
    tri = ((tri_row >= tri_col) | (tri_col >= LANES)).astype(jnp.bfloat16)
    position = lax.broadcasted_iota(jnp.int32, (HALF, CACHE), 1)
    bias = jnp.where(row[:, :1] < 4, bias_ref[0], bias_ref[1])
    wide_lane = lax.broadcasted_iota(jnp.int32, (CACHE, LANES), 1)
    chunks = CACHE // LANES

    copy_q.wait()
    folded = jnp.concatenate([wq_v[: WIDTH // 2], wq_v[WIDTH // 2 :]], axis=1)
    query = jnp.dot(normed, folded, preferred_element_type=jnp.float32)
    query = query[:ROWS, :LANES] + query[ROWS:, LANES:]
    query = query.astype(jnp.bfloat16).astype(jnp.float32)

    def scored(group):
        part = query[group // 2 * HALF : group // 2 * HALF + HALF]
        swapped = pltpu.roll(part, 4, 0)
        upper, under = (swapped, part) if group % 2 else (part, swapped)
        part = jnp.where(row < 4, upper, under)
        turned = pltpu.roll(part, HEAD, 1)
        first, second = jnp.where(row < 4, part, turned), jnp.where(row < 4, turned, part)
        blocks = []
        for p in range(2):
            low = (row % 4 == 2 * p) & (lane < HEAD)
            high = (row % 4 == 2 * p + 1) & (lane >= HEAD)
            blocks.append(jnp.where(low, first, jnp.where(high, second, 0.0)))
            j = group * 4 + 2 * p
            copies[j].wait()
            copies[j + 1].wait()
            even = kv_v[j]
            odd = pltpu.roll(kv_v[j + 1].astype(jnp.float32), HEAD, 1).astype(jnp.bfloat16)
            key_v[group, :, p * LANES : (p + 1) * LANES] = jnp.where(wide_lane < HEAD, even, odd)
            value_v[group, :, p * LANES : (p + 1) * LANES] = jnp.where(wide_lane < HEAD, odd, even)
        lhs = jnp.concatenate(blocks, axis=1).astype(jnp.bfloat16)
        scores = lax.dot_general(lhs, key_v[group], NT, preferred_element_type=jnp.float32)
        return scores * 0.125 + bias

    def attended(group, scores):
        length = jnp.full((HALF, 1), len_ref[group * 4], jnp.int32)
        for j in range(1, 4):
            length = jnp.where(row[:, :1] % 4 == j, len_ref[group * 4 + j], length)
        valid = position < length
        soft = jnp.maximum(scores, 0.0) + jnp.log1p(jnp.exp(-jnp.abs(scores)))
        soft = jnp.where(valid, soft, 0.0)
        stacked = jnp.concatenate(
            [soft[:, c * LANES : (c + 1) * LANES] for c in range(chunks)], axis=0
        )
        high = stacked.astype(jnp.bfloat16)
        rest = stacked - high.astype(jnp.float32)
        middle = rest.astype(jnp.bfloat16)
        low = (rest - middle.astype(jnp.float32)).astype(jnp.bfloat16)
        sums = jnp.dot(
            jnp.concatenate([high, middle, low], axis=0), tri, preferred_element_type=jnp.float32
        )
        size = chunks * HALF
        sums = sums[:size] + sums[size : 2 * size] + sums[2 * size :]
        pieces = [None] * chunks
        carry = jnp.zeros((HALF, LANES), jnp.float32)
        for c in reversed(range(chunks)):
            rows = sums[c * HALF : (c + 1) * HALF]
            pieces[c] = rows[:, :LANES] + carry
            carry = carry + rows[:, LANES:]
        later = jnp.concatenate(pieces, axis=1)
        weights = jnp.where(valid, jnp.exp(scores - later), 0.0).astype(jnp.bfloat16)
        mixed = jnp.dot(weights, value_v[group], preferred_element_type=jnp.float32)
        own = jnp.zeros((HALF, LANES), jnp.float32)
        for p in range(2):
            here = (row % 4 == 2 * p) & (lane >= HEAD)
            here = here | ((row % 4 == 2 * p + 1) & (lane < HEAD))
            own = jnp.where(here, mixed[:, p * LANES : (p + 1) * LANES], own)
        mean = jnp.sum(own * own, axis=-1, keepdims=True) * (1.0 / HEAD)
        own = (own + pltpu.roll(own, HEAD, 1)) * lax.rsqrt(mean + epsilon)
        return jnp.where(lane < HEAD, own, pltpu.roll(own, 4, 0)) * hgain_ref[...]

    scores = scored(0)
    heads = []
    for group in range(4):
        later_scores = scored(group + 1) if group < 3 else None
        heads.append(attended(group, scores))
        scores = later_scores
    head_rows = jnp.concatenate(
        [jnp.where(row < 4, heads[2 * k], pltpu.roll(heads[2 * k + 1], 4, 0)) for k in range(2)],
        axis=0,
    ).astype(jnp.bfloat16)
    copy_o.wait()
    share = jnp.dot(head_rows, wo_v[...], preferred_element_type=jnp.float32)
    out_ref[...] = share.astype(jnp.bfloat16)


def in_hbm(*arrays):
    return [pltpu.with_memory_space_constraint(a, pltpu.HBM) for a in arrays]


def attention(
    tokens, attn_gain, w_query, stick_bias, kv_cache, lengths, head_gain, w_attn_out, routes
):
    return pl.pallas_call(
        attention_kernel,
        out_shape=(
            pltpu.VMEM((ROWS, WIDTH), jnp.bfloat16),
            pltpu.VMEM((4 * ROWS, MESSAGES), jnp.bfloat16),
        ),
        in_specs=[SMEM, SMEM, VMEM, VMEM, VMEM, VMEM] + [HBM] * 3,
        out_specs=(VMEM, VMEM),
        scratch_shapes=[
            pltpu.VMEM((WIDTH, LANES), jnp.bfloat16),
            pltpu.VMEM((ROWS, CACHE, LANES), jnp.bfloat16),
            pltpu.VMEM((4, CACHE, 2 * LANES), jnp.bfloat16),
            pltpu.VMEM((4, CACHE, 2 * LANES), jnp.bfloat16),
            pltpu.VMEM((LANES, WIDTH), jnp.bfloat16),
            pltpu.SemaphoreType.DMA,
            pltpu.SemaphoreType.DMA((ROWS,)),
            pltpu.SemaphoreType.DMA,
        ],
        cost_estimate=pl.CostEstimate(
            flops=400_000_000, bytes_accessed=6_000_000, transcendentals=200_000
        ),
    )(
        lengths, stick_bias, tokens, attn_gain.reshape(1, -1), head_gain.reshape(1, -1), routes.T,
        *in_hbm(w_query, kv_cache, w_attn_out),
    )


def mix_kernel(route_ref, weight_ref, branch_ref, mix_ref):
    shape = (ROWS, RETURNED)
    row = lax.broadcasted_iota(jnp.int32, shape, 0)
    col = lax.broadcasted_iota(jnp.int32, shape, 1)
    device, t = 31 - (col >> 6), 7 - ((col >> 3) & 7)
    kind, slot, side = (col >> 2) & 1, (col >> 1) & 1, col & 1
    first, second = hits_of(route_ref[...], device, slot)
    one, two = columns_of(weight_ref[...])
    expert = jnp.where(first, one, jnp.where(second, two, 0.0))
    dense = jnp.where(row == quarter_of(device, t & 1, slot), branch_ref[:, 0:1], 0.0)
    value = jnp.where(kind == 0, expert, dense)
    both = jnp.concatenate([jnp.where(side == h, value, 0.0) for h in range(2)], axis=0)
    mix_ref[...] = both.astype(jnp.bfloat16)


def mix_table(routes, weights, branch):
    return pl.pallas_call(
        mix_kernel,
        out_shape=jax.ShapeDtypeStruct((2 * ROWS, RETURNED), jnp.bfloat16),
        in_specs=[VMEM, VMEM, VMEM],
        out_specs=VMEM,
        compiler_params=pltpu.CompilerParams(vmem_limit_bytes=8192 * KIB),
        cost_estimate=pl.CostEstimate(
            flops=1_000_000, bytes_accessed=100_000, transcendentals=0
        ),
    )(routes.T, weights.T, branch)


def dispatch_kernel(
    a_ref, b_ref, c_ref, d_ref, tok_ref, gain_ref, gate_ref, pick_ref,
    send_ref, res_ref, branch_ref,
):
    total = a_ref[...].astype(jnp.float32) + b_ref[...].astype(jnp.float32)
    total = total + (c_ref[...].astype(jnp.float32) + d_ref[...].astype(jnp.float32))
    total = total + tok_ref[...].astype(jnp.float32)
    res_ref[...] = total
    scale = lax.rsqrt(jnp.mean(total * total, axis=-1, keepdims=True) + epsilon)
    normed = (total * scale * gain_ref[...]).astype(jnp.bfloat16)
    logit = jnp.sum(
        normed.astype(jnp.float32) * gate_ref[...].astype(jnp.float32), axis=-1, keepdims=True
    )
    branch_ref[...] = jnp.broadcast_to(1.0 / (1.0 + jnp.exp(-logit)), branch_ref.shape)
    stacked = jnp.concatenate([normed[:, q * PART : (q + 1) * PART] for q in range(4)], axis=0)
    send_ref[...] = lax.dot_general(
        pick_ref[...], stacked, (((0,), (0,)), ((), ())), preferred_element_type=jnp.float32
    ).astype(jnp.bfloat16)


def dispatch(shares, tokens, ffn_gain, branch_gate, picks):
    return pl.pallas_call(
        dispatch_kernel,
        out_shape=(
            jax.ShapeDtypeStruct((MESSAGES, PART), jnp.bfloat16),
            jax.ShapeDtypeStruct((ROWS, WIDTH), jnp.float32),
            jax.ShapeDtypeStruct((ROWS, LANES), jnp.float32),
        ),
        in_specs=[VMEM] * 8,
        out_specs=(VMEM, VMEM, VMEM),
        compiler_params=pltpu.CompilerParams(vmem_limit_bytes=8192 * KIB),
        cost_estimate=pl.CostEstimate(
            flops=40_000_000, bytes_accessed=1_500_000, transcendentals=100
        ),
    )(*shares, tokens, ffn_gain.reshape(1, -1), branch_gate.reshape(1, -1), picks)


def feed_kernel(got_ref, eg_hbm, eu_hbm, ed_hbm, *rest):
    packs = rest[:8]
    out_ref, wide_v, back_v, eg_v, eu_v, ed_v, dg_v, du_v, dd_v, e_sem, d_sem = rest[8:]
    expert_copies = [
        pltpu.make_async_copy(src, dst, e_sem.at[k])
        for k, (src, dst) in enumerate(((eg_hbm, eg_v), (eu_hbm, eu_v), (ed_hbm, ed_v)))
    ]
    dense_copies = [
        pltpu.make_async_copy(pack.at[k], dst.at[pl.ds(32 * i, 32), :], d_sem.at[8 * k + i])
        for k, dst in enumerate((dg_v, du_v, dd_v))
        for i, pack in enumerate(packs)
    ]
    for copy in expert_copies + dense_copies:
        copy.start()
    for l in range(4):
        wide_v[l] = got_ref[:, l * LANES : (l + 1) * LANES].astype(jnp.float32)

    def unpacked(kind):
        parts = [
            jnp.concatenate(
                [wide_v[l, pl.ds(kind * 8 + q * 2 + slot, 32, stride=16), :] for slot in range(2)],
                axis=0,
            )
            for q in range(4)
            for l in range(4)
        ]
        return jnp.concatenate(parts, axis=1).astype(jnp.bfloat16)

    def packed(kind, value):
        for t in range(8):
            for slot in range(2):
                for h in range(2):
                    at = t * 256 + h * LANES
                    first = (7 - t) * 8 + kind * 4 + slot * 2 + h
                    back_v[pl.ds(first, 32, stride=64), :] = value[
                        slot * 32 : slot * 32 + 32, at : at + LANES
                    ]

    rows = unpacked(0)
    dense_rows = unpacked(1)
    expert_copies[0].wait()
    a = jnp.dot(rows, eg_v[...], preferred_element_type=jnp.float32)
    expert_copies[1].wait()
    b = jnp.dot(rows, eu_v[...], preferred_element_type=jnp.float32)
    hidden = (a / (1.0 + jnp.exp(-a)) * b).astype(jnp.bfloat16)
    expert_copies[2].wait()
    packed(0, jnp.dot(hidden, ed_v[...], preferred_element_type=jnp.float32))
    for copy in dense_copies[:8]:
        copy.wait()
    a = lax.dot_general(dense_rows, dg_v[...], NT, preferred_element_type=jnp.float32)
    for copy in dense_copies[8:16]:
        copy.wait()
    b = lax.dot_general(dense_rows, du_v[...], NT, preferred_element_type=jnp.float32)
    hidden = (a / (1.0 + jnp.exp(-a)) * b).astype(jnp.bfloat16)
    for copy in dense_copies[16:]:
        copy.wait()
    packed(1, jnp.dot(hidden, dd_v[...], preferred_element_type=jnp.float32))
    out_ref[...] = back_v[...].astype(jnp.bfloat16)


def feed(got, gate, up, down, packs):
    return pl.pallas_call(
        feed_kernel,
        out_shape=jax.ShapeDtypeStruct((RETURNED, LANES), jnp.bfloat16),
        in_specs=[VMEM] + [HBM] * 11,
        out_specs=VMEM,
        scratch_shapes=[
            pltpu.VMEM((4, MESSAGES, LANES), jnp.float32),
            pltpu.VMEM((RETURNED, LANES), jnp.float32),
            pltpu.VMEM((WIDTH, 256), jnp.bfloat16),
            pltpu.VMEM((WIDTH, 256), jnp.bfloat16),
            pltpu.VMEM((256, WIDTH), jnp.bfloat16),
            pltpu.VMEM((256, WIDTH), jnp.bfloat16),
            pltpu.VMEM((256, WIDTH), jnp.bfloat16),
            pltpu.VMEM((256, WIDTH), jnp.bfloat16),
            pltpu.SemaphoreType.DMA((3,)),
            pltpu.SemaphoreType.DMA((24,)),
        ],
        compiler_params=pltpu.CompilerParams(vmem_limit_bytes=24576 * KIB),
        cost_estimate=pl.CostEstimate(
            flops=1_000_000_000, bytes_accessed=7_000_000, transcendentals=40_000
        ),
    )(got, *in_hbm(gate, up, down, *packs))


def finish_kernel(mix_ref, got_ref, res_ref, out_ref):
    total = jnp.dot(mix_ref[...], got_ref[...], preferred_element_type=jnp.float32)
    total = jnp.concatenate([total[:ROWS], total[ROWS:]], axis=1)
    out_ref[...] = (res_ref[...] + total).astype(jnp.bfloat16)


def finish(mix, returned, residual):
    return pl.pallas_call(
        finish_kernel,
        out_shape=jax.ShapeDtypeStruct((ROWS, 256), jnp.bfloat16),
        in_specs=[VMEM] * 3,
        out_specs=VMEM,
        compiler_params=pltpu.CompilerParams(vmem_limit_bytes=8192 * KIB),
        cost_estimate=pl.CostEstimate(
            flops=40_000_000, bytes_accessed=600_000, transcendentals=0
        ),
    )(mix, returned, residual)


def along_y(x, step):
    return lax.ppermute(x, "tp", [(i, (i + 2 * step) % 8) for i in range(8)])


def layer(
    tokens, attn_gain, w_query, stick_bias, kv_cache, lengths, head_gain, w_attn_out, ffn_gain,
    route_expert, route_weight, w_exp_gate, w_exp_up, w_exp_down, branch_gate,
    w_dense_gate, w_dense_up, w_dense_down,
):
    single, half = jnp.float32, jnp.bfloat16
    t = lax.axis_index("tp")
    swap = [(i, i ^ 1) for i in range(8)]

    square = [(i, i ^ 1) for i in range(32)]
    own = lax.optimization_barrier(jnp.stack([w_dense_gate, w_dense_up, w_dense_down]))
    packs = [own, lax.ppermute(own, "ep", [(i, i ^ 4) for i in range(32)])]
    packs.append(lax.ppermute(own, "ep", square))
    share, picks = attention(
        tokens, attn_gain, w_query, stick_bias, kv_cache, lengths, head_gain, w_attn_out,
        route_expert,
    )
    other = lax.ppermute(share, "tp", swap)
    share = (share.astype(single) + other.astype(single)).astype(half)
    shares = [share]
    for step in (1, 3, 2):
        shares.append(along_y(share, step))
    packs.append(lax.ppermute(packs[1], "ep", square))
    send, residual, branch = dispatch(shares, tokens, ffn_gain, branch_gate, picks)
    got = lax.all_to_all(
        send.reshape(32, 16, PART), "ep", 0, 0, tiled=True,
        axis_index_groups=[list(range(31, -1, -1))],
    )

    for k in range(4):
        packs.append(lax.ppermute(packs[k], "tp", swap))
    back = feed(
        got.reshape(MESSAGES, PART), w_exp_gate[0], w_exp_up[0], w_exp_down[0], packs
    )
    returned = lax.all_to_all(
        back.reshape(256, 8, LANES), ("ep", "tp"), 0, 0, tiled=True,
        axis_index_groups=[list(range(255, -1, -1))],
    )
    mix = mix_table(route_expert, route_weight, branch)
    residual_cols = lax.dynamic_slice_in_dim(residual, t * 256, 256, 1)
    return finish(mix, returned.reshape(RETURNED, LANES), residual_cols)


def solution(mesh):
    return jax.shard_map(
        layer,
        mesh=mesh,
        in_specs=(
            P("ep", None), P(), P(None, "tp"), P("tp"), P("ep", "tp", None, None), P("ep"),
            P("tp"), P("tp", None), P(), P("ep", None), P("ep", None), P("ep", None, "tp"),
            P("ep", None, "tp"), P("ep", "tp", None), P(), P(("ep", "tp"), None),
            P(("ep", "tp"), None), P(("ep", "tp"), None),
        ),
        out_specs=P("ep", "tp"),
        check_vma=False,
    )
```

```python
import jax
import jax.numpy as jnp
from jax import lax
from jax.experimental import pallas as pl
from jax.experimental.pallas import tpu as pltpu
from jax.sharding import PartitionSpec as P


HEAD = 64
CACHE = 1024
WIDTH = 2048
ROWS = 16
LANES = 128
HALF = 8
KIB = 1024
MESSAGES = 512
PART = 512
RETURNED = 512
epsilon = 1e-06
NT = (((1,), (1,)), ((), ()))
VMEM = pl.BlockSpec(memory_space=pltpu.VMEM)
SMEM = pl.BlockSpec(memory_space=pltpu.SMEM)
HBM = pl.BlockSpec(memory_space=pltpu.HBM)


def columns_of(pair):
    r = lax.broadcasted_iota(jnp.int32, (ROWS, ROWS), 0)
    c = lax.broadcasted_iota(jnp.int32, (ROWS, ROWS), 1)
    pair = pair.astype(jnp.float32)
    return [
        jnp.sum(jnp.where(r == c, pair[k : k + 1], 0.0), axis=-1, keepdims=True) for k in range(2)
    ]


def hits_of(routes, expert, slot):
    first, second = [expert == c.astype(jnp.int32) for c in columns_of(routes)]
    hit = (first | second).astype(jnp.float32).astype(jnp.bfloat16)
    r = lax.broadcasted_iota(jnp.int32, (ROWS, ROWS), 0)
    c = lax.broadcasted_iota(jnp.int32, (ROWS, ROWS), 1)
    before = jnp.dot(
        (c < r).astype(jnp.float32).astype(jnp.bfloat16), hit, preferred_element_type=jnp.float32
    )
    right = before == slot.astype(jnp.float32)
    return first & right, second & right


def quarter_of(device, core, slot):
    return 4 * (2 * ((device >> 2) & 1) + (device & 1)) + 2 * core + slot


def picks_of(routes):
    core = lax.axis_index("tp") % 2
    shape = (ROWS, MESSAGES)
    row = lax.broadcasted_iota(jnp.int32, shape, 0)
    col = lax.broadcasted_iota(jnp.int32, shape, 1)
    device, kind, q, slot = 31 - (col >> 4), (col >> 3) & 1, (col >> 1) & 3, col & 1
    first, second = hits_of(routes, device, slot)
    expert = (first | second) & (kind == 0)
    dense = (row == quarter_of(device, core, slot)) & (kind == 1)
    pick = jnp.where(expert | dense, 1.0, 0.0)
    stacked = jnp.concatenate([jnp.where(q == k, pick, 0.0) for k in range(4)], axis=0)
    return stacked.astype(jnp.bfloat16)


def attention_kernel(
    len_hbm, bias_hbm, tok_hbm, gain_hbm, hgain_hbm, route_hbm, wq_hbm, kv_hbm, wo_hbm,
    out_ref, pick_ref,
    len_v, bias_v, tok_v, gain_v, hgain_v, route_v,
    wq_v, kv_v, key_v, value_v, wo_v, small_sem, q_sem, kv_sem, o_sem,
):
    smalls = [
        pltpu.make_async_copy(src, dst, small_sem.at[k])
        for k, (src, dst) in enumerate((
            (tok_hbm, tok_v), (gain_hbm, gain_v), (route_hbm, route_v), (len_hbm, len_v),
            (bias_hbm, bias_v), (hgain_hbm, hgain_v),
        ))
    ]
    for copy in smalls:
        copy.start()
    copy_q = pltpu.make_async_copy(wq_hbm, wq_v, q_sem)
    copy_q.start()
    copies = []
    for s in range(ROWS):
        copy = pltpu.make_async_copy(kv_hbm.at[s, 0], kv_v.at[s], kv_sem.at[s])
        copy.start()
        copies.append(copy)
    copy_o = pltpu.make_async_copy(wo_hbm, wo_v, o_sem)
    copy_o.start()
    for copy in smalls:
        copy.wait()
    wide = tok_v[...].astype(jnp.float32)
    scale = lax.rsqrt(jnp.mean(wide * wide, axis=-1, keepdims=True) + epsilon)
    normed = (wide * scale * gain_v[...]).astype(jnp.bfloat16)
    normed = jnp.concatenate([normed[:, : WIDTH // 2], normed[:, WIDTH // 2 :]], axis=0)
    pick_ref[...] = picks_of(route_v[...])

    lane = lax.broadcasted_iota(jnp.int32, (HALF, LANES), 1)
    row = lax.broadcasted_iota(jnp.int32, (HALF, LANES), 0)
    tri_row = lax.broadcasted_iota(jnp.int32, (LANES, 2 * LANES), 0)
    tri_col = lax.broadcasted_iota(jnp.int32, (LANES, 2 * LANES), 1)
    tri = ((tri_row >= tri_col) | (tri_col >= LANES)).astype(jnp.bfloat16)
    position = lax.broadcasted_iota(jnp.int32, (HALF, CACHE), 1)
    bias = jnp.where(row[:, :1] < 4, bias_v[:, 0:1], bias_v[:, 1:2])
    lengths = len_v[...].astype(jnp.float32)
    seq = lax.broadcasted_iota(jnp.int32, (HALF, ROWS), 1)
    seq_row = lax.broadcasted_iota(jnp.int32, (HALF, ROWS), 0) % 4
    wide_lane = lax.broadcasted_iota(jnp.int32, (CACHE, LANES), 1)
    chunks = CACHE // LANES

    copy_q.wait()
    folded = jnp.concatenate([wq_v[: WIDTH // 2], wq_v[WIDTH // 2 :]], axis=1)
    query = jnp.dot(normed, folded, preferred_element_type=jnp.float32)
    query = query[:ROWS, :LANES] + query[ROWS:, LANES:]
    query = query.astype(jnp.bfloat16).astype(jnp.float32)

    def scored(group):
        part = query[group // 2 * HALF : group // 2 * HALF + HALF]
        swapped = pltpu.roll(part, 4, 0)
        upper, under = (swapped, part) if group % 2 else (part, swapped)
        part = jnp.where(row < 4, upper, under)
        turned = pltpu.roll(part, HEAD, 1)
        first, second = jnp.where(row < 4, part, turned), jnp.where(row < 4, turned, part)
        blocks = []
        for p in range(2):
            low = (row % 4 == 2 * p) & (lane < HEAD)
            high = (row % 4 == 2 * p + 1) & (lane >= HEAD)
            blocks.append(jnp.where(low, first, jnp.where(high, second, 0.0)))
            j = group * 4 + 2 * p
            copies[j].wait()
            copies[j + 1].wait()
            even = kv_v[j]
            odd = pltpu.roll(kv_v[j + 1].astype(jnp.float32), HEAD, 1).astype(jnp.bfloat16)
            key_v[group, :, p * LANES : (p + 1) * LANES] = jnp.where(wide_lane < HEAD, even, odd)
            value_v[group, :, p * LANES : (p + 1) * LANES] = jnp.where(wide_lane < HEAD, odd, even)
        lhs = jnp.concatenate(blocks, axis=1).astype(jnp.bfloat16)
        scores = lax.dot_general(lhs, key_v[group], NT, preferred_element_type=jnp.float32)
        return scores * 0.125 + bias

    def attended(group, scores):
        mine = jnp.where(seq == group * 4 + seq_row, lengths, 0.0)
        valid = position < jnp.sum(mine, axis=-1, keepdims=True).astype(jnp.int32)
        soft = jnp.maximum(scores, 0.0) + jnp.log1p(jnp.exp(-jnp.abs(scores)))
        soft = jnp.where(valid, soft, 0.0)
        stacked = jnp.concatenate(
            [soft[:, c * LANES : (c + 1) * LANES] for c in range(chunks)], axis=0
        )
        high = stacked.astype(jnp.bfloat16)
        rest = stacked - high.astype(jnp.float32)
        middle = rest.astype(jnp.bfloat16)
        low = (rest - middle.astype(jnp.float32)).astype(jnp.bfloat16)
        sums = jnp.dot(
            jnp.concatenate([high, middle, low], axis=0), tri, preferred_element_type=jnp.float32
        )
        size = chunks * HALF
        sums = sums[:size] + sums[size : 2 * size] + sums[2 * size :]
        pieces = [None] * chunks
        carry = jnp.zeros((HALF, LANES), jnp.float32)
        for c in reversed(range(chunks)):
            rows = sums[c * HALF : (c + 1) * HALF]
            pieces[c] = rows[:, :LANES] + carry
            carry = carry + rows[:, LANES:]
        later = jnp.concatenate(pieces, axis=1)
        weights = jnp.where(valid, jnp.exp(scores - later), 0.0).astype(jnp.bfloat16)
        mixed = jnp.dot(weights, value_v[group], preferred_element_type=jnp.float32)
        own = jnp.zeros((HALF, LANES), jnp.float32)
        for p in range(2):
            here = (row % 4 == 2 * p) & (lane >= HEAD)
            here = here | ((row % 4 == 2 * p + 1) & (lane < HEAD))
            own = jnp.where(here, mixed[:, p * LANES : (p + 1) * LANES], own)
        mean = jnp.sum(own * own, axis=-1, keepdims=True) * (1.0 / HEAD)
        own = (own + pltpu.roll(own, HEAD, 1)) * lax.rsqrt(mean + epsilon)
        return jnp.where(lane < HEAD, own, pltpu.roll(own, 4, 0)) * hgain_v[...]

    scores = scored(0)
    heads = []
    for group in range(4):
        later_scores = scored(group + 1) if group < 3 else None
        heads.append(attended(group, scores))
        scores = later_scores
    head_rows = jnp.concatenate(
        [jnp.where(row < 4, heads[2 * k], pltpu.roll(heads[2 * k + 1], 4, 0)) for k in range(2)],
        axis=0,
    ).astype(jnp.bfloat16)
    copy_o.wait()
    share = jnp.dot(head_rows, wo_v[...], preferred_element_type=jnp.float32)
    out_ref[...] = share.astype(jnp.bfloat16)


def in_hbm(*arrays):
    return [pltpu.with_memory_space_constraint(a, pltpu.HBM) for a in arrays]


def attention(
    tokens, attn_gain, w_query, stick_bias, kv_cache, lengths, head_gain, w_attn_out, routes
):
    return pl.pallas_call(
        attention_kernel,
        out_shape=(
            pltpu.VMEM((ROWS, WIDTH), jnp.bfloat16),
            pltpu.VMEM((4 * ROWS, MESSAGES), jnp.bfloat16),
        ),
        in_specs=[HBM] * 9,
        out_specs=(VMEM, VMEM),
        scratch_shapes=[
            pltpu.VMEM((1, ROWS), jnp.int32),
            pltpu.VMEM((1, 2), jnp.float32),
            pltpu.VMEM((ROWS, WIDTH), jnp.bfloat16),
            pltpu.VMEM((1, WIDTH), jnp.float32),
            pltpu.VMEM((1, LANES), jnp.float32),
            pltpu.VMEM((2, ROWS), jnp.int32),
            pltpu.VMEM((WIDTH, LANES), jnp.bfloat16),
            pltpu.VMEM((ROWS, CACHE, LANES), jnp.bfloat16),
            pltpu.VMEM((4, CACHE, 2 * LANES), jnp.bfloat16),
            pltpu.VMEM((4, CACHE, 2 * LANES), jnp.bfloat16),
            pltpu.VMEM((LANES, WIDTH), jnp.bfloat16),
            pltpu.SemaphoreType.DMA((6,)),
            pltpu.SemaphoreType.DMA,
            pltpu.SemaphoreType.DMA((ROWS,)),
            pltpu.SemaphoreType.DMA,
        ],
        cost_estimate=pl.CostEstimate(
            flops=400_000_000, bytes_accessed=6_000_000, transcendentals=200_000
        ),
    )(
        *in_hbm(
            lengths.reshape(1, -1), stick_bias.reshape(1, -1), tokens, attn_gain.reshape(1, -1),
            head_gain.reshape(1, -1), routes.T, w_query, kv_cache, w_attn_out,
        ),
    )


def mix_kernel(route_ref, weight_ref, branch_ref, mix_ref):
    shape = (ROWS, RETURNED)
    row = lax.broadcasted_iota(jnp.int32, shape, 0)
    col = lax.broadcasted_iota(jnp.int32, shape, 1)
    device, kind, slot, side = 31 - (col >> 4), (col >> 2) & 3, (col >> 1) & 1, col & 1
    first, second = hits_of(route_ref[...], device, slot)
    one, two = columns_of(weight_ref[...])
    expert = jnp.where(first, one, jnp.where(second, two, 0.0))
    dense = jnp.where(row == quarter_of(device, kind - 1, slot), branch_ref[:, 0:1], 0.0)
    value = jnp.where(kind == 0, expert, jnp.where(kind == 3, 0.0, dense))
    both = jnp.concatenate([jnp.where(side == h, value, 0.0) for h in range(2)], axis=0)
    mix_ref[...] = both.astype(jnp.bfloat16)


def mix_table(routes, weights, branch):
    return pl.pallas_call(
        mix_kernel,
        out_shape=jax.ShapeDtypeStruct((2 * ROWS, RETURNED), jnp.bfloat16),
        in_specs=[VMEM, VMEM, VMEM],
        out_specs=VMEM,
        compiler_params=pltpu.CompilerParams(vmem_limit_bytes=8192 * KIB),
        cost_estimate=pl.CostEstimate(
            flops=1_000_000, bytes_accessed=100_000, transcendentals=0
        ),
    )(routes.T, weights.T, branch)


def dispatch_kernel(
    a_ref, b_ref, c_ref, d_ref, tok_ref, gain_ref, gate_ref, pick_ref,
    send_ref, res_ref, branch_ref, total_v,
):
    total = a_ref[...].astype(jnp.float32) + b_ref[...].astype(jnp.float32)
    total = total + (c_ref[...].astype(jnp.float32) + d_ref[...].astype(jnp.float32))
    total = total + tok_ref[...].astype(jnp.float32)
    total_v[...] = total
    at = pl.multiple_of(lax.axis_index("tp") * 256, 256)
    res_ref[...] = total_v[:, pl.ds(at, 256)]
    scale = lax.rsqrt(jnp.mean(total * total, axis=-1, keepdims=True) + epsilon)
    normed = (total * scale * gain_ref[...]).astype(jnp.bfloat16)
    logit = jnp.sum(
        normed.astype(jnp.float32) * gate_ref[...].astype(jnp.float32), axis=-1, keepdims=True
    )
    branch_ref[...] = jnp.broadcast_to(1.0 / (1.0 + jnp.exp(-logit)), branch_ref.shape)
    stacked = jnp.concatenate([normed[:, q * PART : (q + 1) * PART] for q in range(4)], axis=0)
    send_ref[...] = lax.dot_general(
        pick_ref[...], stacked, (((0,), (0,)), ((), ())), preferred_element_type=jnp.float32
    ).astype(jnp.bfloat16)


def dispatch(shares, tokens, ffn_gain, branch_gate, picks):
    return pl.pallas_call(
        dispatch_kernel,
        out_shape=(
            jax.ShapeDtypeStruct((MESSAGES, PART), jnp.bfloat16),
            jax.ShapeDtypeStruct((ROWS, 256), jnp.float32),
            jax.ShapeDtypeStruct((ROWS, LANES), jnp.float32),
        ),
        in_specs=[VMEM] * 8,
        out_specs=(VMEM, VMEM, VMEM),
        scratch_shapes=[pltpu.VMEM((ROWS, WIDTH), jnp.float32)],
        compiler_params=pltpu.CompilerParams(vmem_limit_bytes=8192 * KIB),
        cost_estimate=pl.CostEstimate(
            flops=40_000_000, bytes_accessed=1_500_000, transcendentals=100
        ),
    )(*shares, tokens, ffn_gain.reshape(1, -1), branch_gate.reshape(1, -1), picks)


def warm_kernel(gate_hbm, up_hbm, gate_out, up_out, sems):
    copies = [
        pltpu.make_async_copy(gate_hbm, gate_out, sems.at[0]),
        pltpu.make_async_copy(up_hbm, up_out, sems.at[1]),
    ]
    for copy in copies:
        copy.start()
    for copy in copies:
        copy.wait()


def warm(gate, up):
    return pl.pallas_call(
        warm_kernel,
        out_shape=(pltpu.VMEM((WIDTH, 256), jnp.bfloat16),) * 2,
        in_specs=[HBM] * 2,
        out_specs=(VMEM, VMEM),
        scratch_shapes=[pltpu.SemaphoreType.DMA((2,))],
        compiler_params=pltpu.CompilerParams(vmem_limit_bytes=4096 * KIB),
        cost_estimate=pl.CostEstimate(
            flops=1_000_000, bytes_accessed=4_000_000, transcendentals=0
        ),
    )(*in_hbm(gate, up))


def feed_kernel(got_ref, eg_ref, eu_ref, ed_hbm, *rest):
    packs = rest[:8]
    keep_ref, send_ref, wide_v, ed_v, dg_v, du_v, dd_v, e_sem, d_sem = rest[8:]
    lower = lax.axis_index("tp") % 2 == 0
    copy_e = pltpu.make_async_copy(ed_hbm, ed_v, e_sem)
    dense_copies = [
        pltpu.make_async_copy(pack.at[k], dst.at[pl.ds(32 * i, 32), :], d_sem.at[8 * k + i])
        for k, dst in enumerate((dg_v, du_v, dd_v))
        for i, pack in enumerate(packs)
    ]
    for copy in [copy_e] + dense_copies:
        copy.start()
    for l in range(4):
        wide_v[l] = got_ref[:, l * LANES : (l + 1) * LANES].astype(jnp.float32)

    def unpacked(kind):
        parts = [
            jnp.concatenate(
                [wide_v[l, pl.ds(kind * 8 + q * 2 + slot, 32, stride=16), :] for slot in range(2)],
                axis=0,
            )
            for q in range(4)
            for l in range(4)
        ]
        return jnp.concatenate(parts, axis=1).astype(jnp.bfloat16)

    def packed(kind, value):
        here = slice(kind * 64, kind * 64 + 64)
        for y in range(4):
            even = value[:, 512 * y : 512 * y + 256]
            odd = value[:, 512 * y + 256 : 512 * y + 512]
            there = slice(256 * y, 256 * y + 256)
            keep_ref[here, there] = jnp.where(lower, even, odd)
            send_ref[here, there] = jnp.where(lower, odd, even).astype(jnp.bfloat16)

    rows = unpacked(0)
    dense_rows = unpacked(1)
    a = jnp.dot(rows, eg_ref[...], preferred_element_type=jnp.float32)
    b = jnp.dot(rows, eu_ref[...], preferred_element_type=jnp.float32)
    hidden = (a / (1.0 + jnp.exp(-a)) * b).astype(jnp.bfloat16)
    copy_e.wait()
    packed(0, jnp.dot(hidden, ed_v[...], preferred_element_type=jnp.float32))
    for copy in dense_copies[:8]:
        copy.wait()
    a = lax.dot_general(dense_rows, dg_v[...], NT, preferred_element_type=jnp.float32)
    for copy in dense_copies[8:16]:
        copy.wait()
    b = lax.dot_general(dense_rows, du_v[...], NT, preferred_element_type=jnp.float32)
    hidden = (a / (1.0 + jnp.exp(-a)) * b).astype(jnp.bfloat16)
    for copy in dense_copies[16:]:
        copy.wait()
    packed(1, jnp.dot(hidden, dd_v[...], preferred_element_type=jnp.float32))


def feed(got, gate, up, down, packs):
    return pl.pallas_call(
        feed_kernel,
        out_shape=(
            jax.ShapeDtypeStruct((128, 1024), jnp.float32),
            jax.ShapeDtypeStruct((128, 1024), jnp.bfloat16),
        ),
        in_specs=[VMEM] * 3 + [HBM] * 9,
        out_specs=(VMEM, VMEM),
        scratch_shapes=[
            pltpu.VMEM((4, MESSAGES, LANES), jnp.float32),
            pltpu.VMEM((256, WIDTH), jnp.bfloat16),
            pltpu.VMEM((256, WIDTH), jnp.bfloat16),
            pltpu.VMEM((256, WIDTH), jnp.bfloat16),
            pltpu.VMEM((256, WIDTH), jnp.bfloat16),
            pltpu.SemaphoreType.DMA,
            pltpu.SemaphoreType.DMA((24,)),
        ],
        compiler_params=pltpu.CompilerParams(vmem_limit_bytes=24576 * KIB),
        cost_estimate=pl.CostEstimate(
            flops=1_000_000_000, bytes_accessed=7_000_000, transcendentals=40_000
        ),
    )(got, gate, up, *in_hbm(down, *packs))


def halve_kernel(keep_ref, got_ref, out_ref, one_ref, two_ref, three_ref, sum_v):
    lower = lax.axis_index("tp") % 2 == 0
    y = lax.axis_index("tp") // 2
    for k in range(4):
        there = slice(256 * k, 256 * k + 256)
        own, other = keep_ref[64:, there], got_ref[64:, there].astype(jnp.float32)
        sum_v[k, :64] = keep_ref[:64, there] + got_ref[:64, there].astype(jnp.float32)
        sum_v[k, 64:128] = jnp.where(lower, own, other)
        sum_v[k, 128:] = jnp.where(lower, other, own)
    out_ref[...] = sum_v[y]
    for step, ref in ((1, one_ref), (2, two_ref), (3, three_ref)):
        ref[...] = sum_v[(y + step) % 4].astype(jnp.bfloat16)


def halve(keep, got):
    return pl.pallas_call(
        halve_kernel,
        out_shape=(jax.ShapeDtypeStruct((192, 256), jnp.float32),)
        + (jax.ShapeDtypeStruct((192, 256), jnp.bfloat16),) * 3,
        in_specs=[VMEM] * 2,
        out_specs=(VMEM,) * 4,
        scratch_shapes=[pltpu.VMEM((4, 192, 256), jnp.float32)],
        compiler_params=pltpu.CompilerParams(vmem_limit_bytes=8192 * KIB),
        cost_estimate=pl.CostEstimate(
            flops=1_000_000, bytes_accessed=1_000_000, transcendentals=0
        ),
    )(keep, got)


def pack_kernel(a_ref, b_ref, c_ref, d_ref, out_ref, back_v):
    total = a_ref[...] + b_ref[...].astype(jnp.float32)
    total = total + (c_ref[...].astype(jnp.float32) + d_ref[...].astype(jnp.float32))
    for kind in range(4):
        for slot in range(2):
            for h in range(2):
                at = kind * 64 + slot * 32
                if kind < 3:
                    piece = total[at : at + 32, h * LANES : (h + 1) * LANES]
                else:
                    piece = jnp.zeros((32, LANES), jnp.float32)
                back_v[pl.ds(kind * 4 + slot * 2 + h, 32, stride=16), :] = piece
    out_ref[...] = back_v[...].astype(jnp.bfloat16)


def pack(blocks):
    return pl.pallas_call(
        pack_kernel,
        out_shape=jax.ShapeDtypeStruct((RETURNED, LANES), jnp.bfloat16),
        in_specs=[VMEM] * 4,
        out_specs=VMEM,
        scratch_shapes=[pltpu.VMEM((RETURNED, LANES), jnp.float32)],
        compiler_params=pltpu.CompilerParams(vmem_limit_bytes=8192 * KIB),
        cost_estimate=pl.CostEstimate(
            flops=1_000_000, bytes_accessed=500_000, transcendentals=0
        ),
    )(*blocks)


def finish_kernel(mix_ref, got_ref, res_ref, out_ref):
    total = jnp.dot(mix_ref[...], got_ref[...], preferred_element_type=jnp.float32)
    total = jnp.concatenate([total[:ROWS], total[ROWS:]], axis=1)
    out_ref[...] = (res_ref[...] + total).astype(jnp.bfloat16)


def finish(mix, returned, residual):
    return pl.pallas_call(
        finish_kernel,
        out_shape=jax.ShapeDtypeStruct((ROWS, 256), jnp.bfloat16),
        in_specs=[VMEM] * 3,
        out_specs=VMEM,
        compiler_params=pltpu.CompilerParams(vmem_limit_bytes=8192 * KIB),
        cost_estimate=pl.CostEstimate(
            flops=40_000_000, bytes_accessed=600_000, transcendentals=0
        ),
    )(mix, returned, residual)


def along_y(x, step):
    return lax.ppermute(x, "tp", [(i, (i + 2 * step) % 8) for i in range(8)])


def layer(
    tokens, attn_gain, w_query, stick_bias, kv_cache, lengths, head_gain, w_attn_out, ffn_gain,
    route_expert, route_weight, w_exp_gate, w_exp_up, w_exp_down, branch_gate,
    w_dense_gate, w_dense_up, w_dense_down,
):
    single, half = jnp.float32, jnp.bfloat16
    swap = [(i, i ^ 1) for i in range(8)]

    square = [(i, i ^ 1) for i in range(32)]
    own = lax.optimization_barrier(jnp.stack([w_dense_gate, w_dense_up, w_dense_down]))
    packs = [own, lax.ppermute(own, "ep", [(i, i ^ 4) for i in range(32)])]
    packs.append(lax.ppermute(own, "ep", square))
    share, picks = attention(
        tokens, attn_gain, w_query, stick_bias, kv_cache, lengths, head_gain, w_attn_out,
        route_expert,
    )
    other = lax.ppermute(share, "tp", swap)
    share = (share.astype(single) + other.astype(single)).astype(half)
    shares = [share]
    for step in (1, 3, 2):
        shares.append(along_y(share, step))
    packs.append(lax.ppermute(packs[1], "ep", square))
    send, residual, branch = dispatch(shares, tokens, ffn_gain, branch_gate, picks)
    got = lax.all_to_all(
        send.reshape(32, 16, PART), "ep", 0, 0, tiled=True,
        axis_index_groups=[list(range(31, -1, -1))],
    )

    for k in range(4):
        packs.append(lax.ppermute(packs[k], "tp", swap))
    mix = mix_table(route_expert, route_weight, branch)
    gate, up = warm(w_exp_gate[0], w_exp_up[0])
    keep, give = feed(got.reshape(MESSAGES, PART), gate, up, w_exp_down[0], packs)
    taken = lax.ppermute(give, "tp", swap)
    mine, *others = halve(keep, taken)
    blocks = [mine]
    for step in (1, 3, 2):
        blocks.append(along_y(others[step - 1], step))
    back = pack(blocks)
    returned = lax.all_to_all(
        back.reshape(32, 16, LANES), "ep", 0, 0, tiled=True,
        axis_index_groups=[list(range(31, -1, -1))],
    )
    return finish(mix, returned.reshape(RETURNED, LANES), residual)


def solution(mesh):
    return jax.shard_map(
        layer,
        mesh=mesh,
        in_specs=(
            P("ep", None), P(), P(None, "tp"), P("tp"), P("ep", "tp", None, None), P("ep"),
            P("tp"), P("tp", None), P(), P("ep", None), P("ep", None), P("ep", None, "tp"),
            P("ep", None, "tp"), P("ep", "tp", None), P(), P(("ep", "tp"), None),
            P(("ep", "tp"), None), P(("ep", "tp"), None),
        ),
        out_specs=P("ep", "tp"),
        check_vma=False,
    )
```

```python
import jax
import jax.numpy as jnp
from jax import lax
from jax.experimental import pallas as pl
from jax.experimental.pallas import tpu as pltpu
from jax.sharding import PartitionSpec as P


HEAD = 64
CACHE = 1024
WIDTH = 2048
ROWS = 16
LANES = 128
HALF = 8
KIB = 1024
MESSAGES = 768
PART = 256
EACH = 24
RETURNED = 512
epsilon = 1e-06
NT = (((1,), (1,)), ((), ()))
VMEM = pl.BlockSpec(memory_space=pltpu.VMEM)
SMEM = pl.BlockSpec(memory_space=pltpu.SMEM)
HBM = pl.BlockSpec(memory_space=pltpu.HBM)


def columns_of(pair):
    r = lax.broadcasted_iota(jnp.int32, (ROWS, ROWS), 0)
    c = lax.broadcasted_iota(jnp.int32, (ROWS, ROWS), 1)
    pair = pair.astype(jnp.float32)
    return [
        jnp.sum(jnp.where(r == c, pair[k : k + 1], 0.0), axis=-1, keepdims=True) for k in range(2)
    ]


def hits_of(routes, expert, slot):
    first, second = [expert == c.astype(jnp.int32) for c in columns_of(routes)]
    hit = (first | second).astype(jnp.float32).astype(jnp.bfloat16)
    r = lax.broadcasted_iota(jnp.int32, (ROWS, ROWS), 0)
    c = lax.broadcasted_iota(jnp.int32, (ROWS, ROWS), 1)
    before = jnp.dot(
        (c < r).astype(jnp.float32).astype(jnp.bfloat16), hit, preferred_element_type=jnp.float32
    )
    right = before == slot.astype(jnp.float32)
    return first & right, second & right


def quarter_of(device):
    return 4 * (2 * ((device >> 2) & 1) + (device & 1))


def picks_of(routes):
    shape = (ROWS, MESSAGES)
    row = lax.broadcasted_iota(jnp.int32, shape, 0)
    col = lax.broadcasted_iota(jnp.int32, shape, 1)
    block = jnp.zeros(shape, jnp.int32)
    for k in range(1, 32):
        block = block + (col >= k * EACH).astype(jnp.int32)
    inner = col - block * EACH
    q = jnp.zeros(shape, jnp.int32)
    for k in range(1, 4):
        q = q + (inner >= k * 6).astype(jnp.int32)
    place, device = inner - 6 * q, 31 - block
    first, second = hits_of(routes, device, place)
    expert = (first | second) & (place < 2)
    dense = (row == quarter_of(device) + place - 2) & (place >= 2)
    pick = jnp.where(expert | dense, 1.0, 0.0)
    stacked = jnp.concatenate([jnp.where(q == k, pick, 0.0) for k in range(4)], axis=0)
    return stacked.astype(jnp.bfloat16)


def attention_kernel(
    len_hbm, bias_hbm, tok_hbm, gain_hbm, hgain_hbm, route_hbm, wq_hbm, kv_hbm, wo_hbm,
    out_ref, pick_ref,
    len_v, bias_v, tok_v, gain_v, hgain_v, route_v,
    wq_v, kv_v, key_v, value_v, wo_v, small_sem, q_sem, kv_sem, o_sem,
):
    smalls = [
        pltpu.make_async_copy(src, dst, small_sem.at[k])
        for k, (src, dst) in enumerate((
            (tok_hbm, tok_v), (gain_hbm, gain_v), (route_hbm, route_v), (len_hbm, len_v),
            (bias_hbm, bias_v), (hgain_hbm, hgain_v),
        ))
    ]
    for copy in smalls:
        copy.start()
    copy_q = pltpu.make_async_copy(wq_hbm, wq_v, q_sem)
    copy_q.start()
    copies = []
    for s in range(ROWS):
        copy = pltpu.make_async_copy(kv_hbm.at[s, 0], kv_v.at[s], kv_sem.at[s])
        copy.start()
        copies.append(copy)
    copy_o = pltpu.make_async_copy(wo_hbm, wo_v, o_sem)
    copy_o.start()
    for copy in smalls:
        copy.wait()
    wide = tok_v[...].astype(jnp.float32)
    scale = lax.rsqrt(jnp.mean(wide * wide, axis=-1, keepdims=True) + epsilon)
    normed = (wide * scale * gain_v[...]).astype(jnp.bfloat16)
    normed = jnp.concatenate([normed[:, : WIDTH // 2], normed[:, WIDTH // 2 :]], axis=0)
    pick_ref[...] = picks_of(route_v[...])

    lane = lax.broadcasted_iota(jnp.int32, (HALF, LANES), 1)
    row = lax.broadcasted_iota(jnp.int32, (HALF, LANES), 0)
    tri_row = lax.broadcasted_iota(jnp.int32, (LANES, 2 * LANES), 0)
    tri_col = lax.broadcasted_iota(jnp.int32, (LANES, 2 * LANES), 1)
    tri = ((tri_row >= tri_col) | (tri_col >= LANES)).astype(jnp.bfloat16)
    position = lax.broadcasted_iota(jnp.int32, (HALF, CACHE), 1)
    bias = jnp.where(row[:, :1] < 4, bias_v[:, 0:1], bias_v[:, 1:2])
    lengths = len_v[...].astype(jnp.float32)
    seq = lax.broadcasted_iota(jnp.int32, (HALF, ROWS), 1)
    seq_row = lax.broadcasted_iota(jnp.int32, (HALF, ROWS), 0) % 4
    wide_lane = lax.broadcasted_iota(jnp.int32, (CACHE, LANES), 1)
    chunks = CACHE // LANES

    copy_q.wait()
    folded = jnp.concatenate([wq_v[: WIDTH // 2], wq_v[WIDTH // 2 :]], axis=1)
    query = jnp.dot(normed, folded, preferred_element_type=jnp.float32)
    query = query[:ROWS, :LANES] + query[ROWS:, LANES:]
    query = query.astype(jnp.bfloat16).astype(jnp.float32)

    def scored(group):
        part = query[group // 2 * HALF : group // 2 * HALF + HALF]
        swapped = pltpu.roll(part, 4, 0)
        upper, under = (swapped, part) if group % 2 else (part, swapped)
        part = jnp.where(row < 4, upper, under)
        turned = pltpu.roll(part, HEAD, 1)
        first, second = jnp.where(row < 4, part, turned), jnp.where(row < 4, turned, part)
        blocks = []
        for p in range(2):
            low = (row % 4 == 2 * p) & (lane < HEAD)
            high = (row % 4 == 2 * p + 1) & (lane >= HEAD)
            blocks.append(jnp.where(low, first, jnp.where(high, second, 0.0)))
            j = group * 4 + 2 * p
            copies[j].wait()
            copies[j + 1].wait()
            even = kv_v[j]
            odd = pltpu.roll(kv_v[j + 1].astype(jnp.float32), HEAD, 1).astype(jnp.bfloat16)
            key_v[group, :, p * LANES : (p + 1) * LANES] = jnp.where(wide_lane < HEAD, even, odd)
            value_v[group, :, p * LANES : (p + 1) * LANES] = jnp.where(wide_lane < HEAD, odd, even)
        lhs = jnp.concatenate(blocks, axis=1).astype(jnp.bfloat16)
        scores = lax.dot_general(lhs, key_v[group], NT, preferred_element_type=jnp.float32)
        return scores * 0.125 + bias

    def attended(group, scores):
        mine = jnp.where(seq == group * 4 + seq_row, lengths, 0.0)
        valid = position < jnp.sum(mine, axis=-1, keepdims=True).astype(jnp.int32)
        soft = jnp.maximum(scores, 0.0) + jnp.log1p(jnp.exp(-jnp.abs(scores)))
        soft = jnp.where(valid, soft, 0.0)
        stacked = jnp.concatenate(
            [soft[:, c * LANES : (c + 1) * LANES] for c in range(chunks)], axis=0
        )
        high = stacked.astype(jnp.bfloat16)
        rest = stacked - high.astype(jnp.float32)
        middle = rest.astype(jnp.bfloat16)
        low = (rest - middle.astype(jnp.float32)).astype(jnp.bfloat16)
        sums = jnp.dot(
            jnp.concatenate([high, middle, low], axis=0), tri, preferred_element_type=jnp.float32
        )
        size = chunks * HALF
        sums = sums[:size] + sums[size : 2 * size] + sums[2 * size :]
        pieces = [None] * chunks
        carry = jnp.zeros((HALF, LANES), jnp.float32)
        for c in reversed(range(chunks)):
            rows = sums[c * HALF : (c + 1) * HALF]
            pieces[c] = rows[:, :LANES] + carry
            carry = carry + rows[:, LANES:]
        later = jnp.concatenate(pieces, axis=1)
        weights = jnp.where(valid, jnp.exp(scores - later), 0.0).astype(jnp.bfloat16)
        mixed = jnp.dot(weights, value_v[group], preferred_element_type=jnp.float32)
        own = jnp.zeros((HALF, LANES), jnp.float32)
        for p in range(2):
            here = (row % 4 == 2 * p) & (lane >= HEAD)
            here = here | ((row % 4 == 2 * p + 1) & (lane < HEAD))
            own = jnp.where(here, mixed[:, p * LANES : (p + 1) * LANES], own)
        mean = jnp.sum(own * own, axis=-1, keepdims=True) * (1.0 / HEAD)
        own = (own + pltpu.roll(own, HEAD, 1)) * lax.rsqrt(mean + epsilon)
        return jnp.where(lane < HEAD, own, pltpu.roll(own, 4, 0)) * hgain_v[...]

    scores = scored(0)
    heads = []
    for group in range(4):
        later_scores = scored(group + 1) if group < 3 else None
        heads.append(attended(group, scores))
        scores = later_scores
    head_rows = jnp.concatenate(
        [jnp.where(row < 4, heads[2 * k], pltpu.roll(heads[2 * k + 1], 4, 0)) for k in range(2)],
        axis=0,
    ).astype(jnp.bfloat16)
    copy_o.wait()
    share = jnp.dot(head_rows, wo_v[...], preferred_element_type=jnp.float32)
    out_ref[...] = share.astype(jnp.bfloat16)


def in_hbm(*arrays):
    return [pltpu.with_memory_space_constraint(a, pltpu.HBM) for a in arrays]


def attention(
    tokens, attn_gain, w_query, stick_bias, kv_cache, lengths, head_gain, w_attn_out, routes
):
    return pl.pallas_call(
        attention_kernel,
        out_shape=(
            pltpu.VMEM((ROWS, WIDTH), jnp.bfloat16),
            pltpu.VMEM((4 * ROWS, MESSAGES), jnp.bfloat16),
        ),
        in_specs=[HBM] * 9,
        out_specs=(VMEM, VMEM),
        scratch_shapes=[
            pltpu.VMEM((1, ROWS), jnp.int32),
            pltpu.VMEM((1, 2), jnp.float32),
            pltpu.VMEM((ROWS, WIDTH), jnp.bfloat16),
            pltpu.VMEM((1, WIDTH), jnp.float32),
            pltpu.VMEM((1, LANES), jnp.float32),
            pltpu.VMEM((2, ROWS), jnp.int32),
            pltpu.VMEM((WIDTH, LANES), jnp.bfloat16),
            pltpu.VMEM((ROWS, CACHE, LANES), jnp.bfloat16),
            pltpu.VMEM((4, CACHE, 2 * LANES), jnp.bfloat16),
            pltpu.VMEM((4, CACHE, 2 * LANES), jnp.bfloat16),
            pltpu.VMEM((LANES, WIDTH), jnp.bfloat16),
            pltpu.SemaphoreType.DMA((6,)),
            pltpu.SemaphoreType.DMA,
            pltpu.SemaphoreType.DMA((ROWS,)),
            pltpu.SemaphoreType.DMA,
        ],
        cost_estimate=pl.CostEstimate(
            flops=400_000_000, bytes_accessed=6_000_000, transcendentals=200_000
        ),
    )(
        *in_hbm(
            lengths.reshape(1, -1), stick_bias.reshape(1, -1), tokens, attn_gain.reshape(1, -1),
            head_gain.reshape(1, -1), routes.T, w_query, kv_cache, w_attn_out,
        ),
    )


def mix_kernel(route_ref, weight_ref, branch_ref, mix_ref):
    shape = (ROWS, RETURNED)
    row = lax.broadcasted_iota(jnp.int32, shape, 0)
    col = lax.broadcasted_iota(jnp.int32, shape, 1)
    device, place, side = 31 - (col >> 4), (col >> 1) & 7, col & 1
    first, second = hits_of(route_ref[...], device, place)
    one, two = columns_of(weight_ref[...])
    expert = jnp.where(first, one, jnp.where(second, two, 0.0))
    here = (row == quarter_of(device) + place - 2) & (place < 6)
    dense = jnp.where(here, branch_ref[:, 0:1], 0.0)
    value = jnp.where(place < 2, expert, dense)
    both = jnp.concatenate([jnp.where(side == h, value, 0.0) for h in range(2)], axis=0)
    mix_ref[...] = both.astype(jnp.bfloat16)


def mix_table(routes, weights, branch):
    return pl.pallas_call(
        mix_kernel,
        out_shape=jax.ShapeDtypeStruct((2 * ROWS, RETURNED), jnp.bfloat16),
        in_specs=[VMEM, VMEM, VMEM],
        out_specs=VMEM,
        compiler_params=pltpu.CompilerParams(vmem_limit_bytes=8192 * KIB),
        cost_estimate=pl.CostEstimate(
            flops=1_000_000, bytes_accessed=100_000, transcendentals=0
        ),
    )(routes.T, weights.T, branch)


def dispatch_kernel(
    a_ref, b_ref, c_ref, d_ref, tok_ref, gain_ref, gate_ref, pick_ref,
    send_ref, res_ref, branch_ref, total_v,
):
    total = a_ref[...].astype(jnp.float32) + b_ref[...].astype(jnp.float32)
    total = total + (c_ref[...].astype(jnp.float32) + d_ref[...].astype(jnp.float32))
    total = total + tok_ref[...].astype(jnp.float32)
    total_v[...] = total
    at = pl.multiple_of(lax.axis_index("tp") * 256, 256)
    res_ref[...] = total_v[:, pl.ds(at, 256)]
    scale = lax.rsqrt(jnp.mean(total * total, axis=-1, keepdims=True) + epsilon)
    normed = (total * scale * gain_ref[...]).astype(jnp.bfloat16)
    logit = jnp.sum(
        normed.astype(jnp.float32) * gate_ref[...].astype(jnp.float32), axis=-1, keepdims=True
    )
    branch_ref[...] = jnp.broadcast_to(1.0 / (1.0 + jnp.exp(-logit)), branch_ref.shape)
    lower = lax.axis_index("tp") % 2 == 0
    normed = jnp.where(
        lower, normed[:, : WIDTH // 2].astype(jnp.float32), normed[:, WIDTH // 2 :].astype(jnp.float32)
    ).astype(jnp.bfloat16)
    stacked = jnp.concatenate([normed[:, q * PART : (q + 1) * PART] for q in range(4)], axis=0)
    send_ref[...] = lax.dot_general(
        pick_ref[...], stacked, (((0,), (0,)), ((), ())), preferred_element_type=jnp.float32
    ).astype(jnp.bfloat16)


def dispatch(shares, tokens, ffn_gain, branch_gate, picks):
    return pl.pallas_call(
        dispatch_kernel,
        out_shape=(
            jax.ShapeDtypeStruct((MESSAGES, PART), jnp.bfloat16),
            jax.ShapeDtypeStruct((ROWS, 256), jnp.float32),
            jax.ShapeDtypeStruct((ROWS, LANES), jnp.float32),
        ),
        in_specs=[VMEM] * 8,
        out_specs=(VMEM, VMEM, VMEM),
        scratch_shapes=[pltpu.VMEM((ROWS, WIDTH), jnp.float32)],
        compiler_params=pltpu.CompilerParams(vmem_limit_bytes=8192 * KIB),
        cost_estimate=pl.CostEstimate(
            flops=40_000_000, bytes_accessed=1_500_000, transcendentals=100
        ),
    )(*shares, tokens, ffn_gain.reshape(1, -1), branch_gate.reshape(1, -1), picks)


def warm_kernel(gate_hbm, up_hbm, gate_out, up_out, sems):
    copies = [
        pltpu.make_async_copy(gate_hbm, gate_out, sems.at[0]),
        pltpu.make_async_copy(up_hbm, up_out, sems.at[1]),
    ]
    for copy in copies:
        copy.start()
    for copy in copies:
        copy.wait()


def warm(gate, up):
    return pl.pallas_call(
        warm_kernel,
        out_shape=(pltpu.VMEM((WIDTH, 256), jnp.bfloat16),) * 2,
        in_specs=[HBM] * 2,
        out_specs=(VMEM, VMEM),
        scratch_shapes=[pltpu.SemaphoreType.DMA((2,))],
        compiler_params=pltpu.CompilerParams(vmem_limit_bytes=4096 * KIB),
        cost_estimate=pl.CostEstimate(
            flops=1_000_000, bytes_accessed=4_000_000, transcendentals=0
        ),
    )(*in_hbm(gate, up))


def feed_kernel(got_ref, other_ref, eg_ref, eu_ref, ed_hbm, *rest):
    packs = rest[:4]
    keep_ref, send_ref, wide_v, ed_v, both_v, dd_v, e_sem, d_sem = rest[4:]
    lower = lax.axis_index("tp") % 2 == 0
    copy_e = pltpu.make_async_copy(ed_hbm, ed_v, e_sem)
    targets = ((both_v, 0), (both_v, 128), (dd_v, 0))
    dense_copies = [
        pltpu.make_async_copy(
            pack.at[k], dst.at[pl.ds(at + 32 * i, 32), :], d_sem.at[4 * k + i]
        )
        for k, (dst, at) in enumerate(targets)
        for i, pack in enumerate(packs)
    ]
    for copy in [copy_e] + dense_copies:
        copy.start()
    for l in range(2):
        mine = got_ref[:, l * LANES : (l + 1) * LANES].astype(jnp.float32)
        theirs = other_ref[:, l * LANES : (l + 1) * LANES].astype(jnp.float32)
        wide_v[l] = jnp.where(lower, mine, theirs)
        wide_v[2 + l] = jnp.where(lower, theirs, mine)

    def unpacked(places):
        parts = [
            jnp.concatenate(
                [wide_v[2 * s + l, pl.ds(q * 6 + j, 32, stride=EACH), :] for j in places], axis=0
            )
            for s in range(2)
            for q in range(4)
            for l in range(2)
        ]
        return jnp.concatenate(parts, axis=1).astype(jnp.bfloat16)

    def packed(first, value):
        here = slice(first, first + value.shape[0])
        for y in range(4):
            even = value[:, 512 * y : 512 * y + 256]
            odd = value[:, 512 * y + 256 : 512 * y + 512]
            there = slice(256 * y, 256 * y + 256)
            keep_ref[here, there] = jnp.where(lower, even, odd)
            send_ref[here, there] = jnp.where(lower, odd, even).astype(jnp.bfloat16)

    rows = unpacked((0, 1))
    dense_rows = unpacked((2, 3, 4, 5))
    a = jnp.dot(rows, eg_ref[...], preferred_element_type=jnp.float32)
    b = jnp.dot(rows, eu_ref[...], preferred_element_type=jnp.float32)
    hidden = (a / (1.0 + jnp.exp(-a)) * b).astype(jnp.bfloat16)
    copy_e.wait()
    packed(0, jnp.dot(hidden, ed_v[...], preferred_element_type=jnp.float32))
    for copy in dense_copies[:8]:
        copy.wait()
    both = lax.dot_general(dense_rows, both_v[...], NT, preferred_element_type=jnp.float32)
    a, b = both[:, :128], both[:, 128:]
    hidden = (a / (1.0 + jnp.exp(-a)) * b).astype(jnp.bfloat16)
    for copy in dense_copies[8:]:
        copy.wait()
    packed(64, jnp.dot(hidden, dd_v[...], preferred_element_type=jnp.float32))


def feed(got, other, gate, up, down, packs):
    return pl.pallas_call(
        feed_kernel,
        out_shape=(
            jax.ShapeDtypeStruct((192, 1024), jnp.float32),
            jax.ShapeDtypeStruct((192, 1024), jnp.bfloat16),
        ),
        in_specs=[VMEM] * 4 + [HBM] * 5,
        out_specs=(VMEM, VMEM),
        scratch_shapes=[
            pltpu.VMEM((4, MESSAGES, LANES), jnp.float32),
            pltpu.VMEM((256, WIDTH), jnp.bfloat16),
            pltpu.VMEM((256, WIDTH), jnp.bfloat16),
            pltpu.VMEM((128, WIDTH), jnp.bfloat16),
            pltpu.SemaphoreType.DMA,
            pltpu.SemaphoreType.DMA((12,)),
        ],
        compiler_params=pltpu.CompilerParams(vmem_limit_bytes=24576 * KIB),
        cost_estimate=pl.CostEstimate(
            flops=1_000_000_000, bytes_accessed=7_000_000, transcendentals=40_000
        ),
    )(got, other, gate, up, *in_hbm(down), *packs)


def halve_kernel(keep_ref, got_ref, out_ref, one_ref, two_ref, three_ref, sum_v):
    y = lax.axis_index("tp") // 2
    for k in range(4):
        there = slice(256 * k, 256 * k + 256)
        sum_v[k] = keep_ref[:, there] + got_ref[:, there].astype(jnp.float32)
    out_ref[...] = sum_v[y]
    for step, ref in ((1, one_ref), (2, two_ref), (3, three_ref)):
        ref[...] = sum_v[(y + step) % 4].astype(jnp.bfloat16)


def halve(keep, got):
    return pl.pallas_call(
        halve_kernel,
        out_shape=(jax.ShapeDtypeStruct((192, 256), jnp.float32),)
        + (jax.ShapeDtypeStruct((192, 256), jnp.bfloat16),) * 3,
        in_specs=[VMEM] * 2,
        out_specs=(VMEM,) * 4,
        scratch_shapes=[pltpu.VMEM((4, 192, 256), jnp.float32)],
        compiler_params=pltpu.CompilerParams(vmem_limit_bytes=8192 * KIB),
        cost_estimate=pl.CostEstimate(
            flops=1_000_000, bytes_accessed=1_000_000, transcendentals=0
        ),
    )(keep, got)


def pack_kernel(a_ref, b_ref, c_ref, d_ref, out_ref, back_v):
    total = a_ref[...] + b_ref[...].astype(jnp.float32)
    total = total + (c_ref[...].astype(jnp.float32) + d_ref[...].astype(jnp.float32))
    for place in range(8):
        for h in range(2):
            if place < 6:
                piece = total[place * 32 : place * 32 + 32, h * LANES : (h + 1) * LANES]
            else:
                piece = jnp.zeros((32, LANES), jnp.float32)
            back_v[pl.ds(place * 2 + h, 32, stride=16), :] = piece
    out_ref[...] = back_v[...].astype(jnp.bfloat16)


def pack(blocks):
    return pl.pallas_call(
        pack_kernel,
        out_shape=jax.ShapeDtypeStruct((RETURNED, LANES), jnp.bfloat16),
        in_specs=[VMEM] * 4,
        out_specs=VMEM,
        scratch_shapes=[pltpu.VMEM((RETURNED, LANES), jnp.float32)],
        compiler_params=pltpu.CompilerParams(vmem_limit_bytes=8192 * KIB),
        cost_estimate=pl.CostEstimate(
            flops=1_000_000, bytes_accessed=500_000, transcendentals=0
        ),
    )(*blocks)


def finish_kernel(mix_ref, got_ref, res_ref, out_ref):
    total = jnp.dot(mix_ref[...], got_ref[...], preferred_element_type=jnp.float32)
    total = jnp.concatenate([total[:ROWS], total[ROWS:]], axis=1)
    out_ref[...] = (res_ref[...] + total).astype(jnp.bfloat16)


def finish(mix, returned, residual):
    return pl.pallas_call(
        finish_kernel,
        out_shape=jax.ShapeDtypeStruct((ROWS, 256), jnp.bfloat16),
        in_specs=[VMEM] * 3,
        out_specs=VMEM,
        compiler_params=pltpu.CompilerParams(vmem_limit_bytes=8192 * KIB),
        cost_estimate=pl.CostEstimate(
            flops=40_000_000, bytes_accessed=600_000, transcendentals=0
        ),
    )(mix, returned, residual)


def along_y(x, step):
    return lax.ppermute(x, "tp", [(i, (i + 2 * step) % 8) for i in range(8)])


def layer(
    tokens, attn_gain, w_query, stick_bias, kv_cache, lengths, head_gain, w_attn_out, ffn_gain,
    route_expert, route_weight, w_exp_gate, w_exp_up, w_exp_down, branch_gate,
    w_dense_gate, w_dense_up, w_dense_down,
):
    single, half = jnp.float32, jnp.bfloat16
    swap = [(i, i ^ 1) for i in range(8)]

    square = [(i, i ^ 1) for i in range(32)]
    own = lax.optimization_barrier(jnp.stack([w_dense_gate, w_dense_up, w_dense_down]))
    packs = [own, lax.ppermute(own, "ep", [(i, i ^ 4) for i in range(32)])]
    packs.append(lax.ppermute(own, "ep", square))
    share, picks = attention(
        tokens, attn_gain, w_query, stick_bias, kv_cache, lengths, head_gain, w_attn_out,
        route_expert,
    )
    other = lax.ppermute(share, "tp", swap)
    share = (share.astype(single) + other.astype(single)).astype(half)
    shares = [share]
    for step in (1, 3, 2):
        shares.append(along_y(share, step))
    packs.append(lax.ppermute(packs[1], "ep", square))
    send, residual, branch = dispatch(shares, tokens, ffn_gain, branch_gate, picks)
    got = lax.all_to_all(
        send.reshape(32, EACH, PART), "ep", 0, 0, tiled=True,
        axis_index_groups=[list(range(31, -1, -1))],
    )

    mix = mix_table(route_expert, route_weight, branch)
    gate, up = warm(w_exp_gate[0], w_exp_up[0])
    got = got.reshape(MESSAGES, PART)
    other = lax.ppermute(got, "tp", swap)
    keep, give = feed(got, other, gate, up, w_exp_down[0], packs)
    taken = lax.ppermute(give, "tp", swap)
    mine, *others = halve(keep, taken)
    blocks = [mine]
    for step in (1, 3, 2):
        blocks.append(along_y(others[step - 1], step))
    back = pack(blocks)
    returned = lax.all_to_all(
        back.reshape(32, 16, LANES), "ep", 0, 0, tiled=True,
        axis_index_groups=[list(range(31, -1, -1))],
    )
    return finish(mix, returned.reshape(RETURNED, LANES), residual)


def solution(mesh):
    return jax.shard_map(
        layer,
        mesh=mesh,
        in_specs=(
            P("ep", None), P(), P(None, "tp"), P("tp"), P("ep", "tp", None, None), P("ep"),
            P("tp"), P("tp", None), P(), P("ep", None), P("ep", None), P("ep", None, "tp"),
            P("ep", None, "tp"), P("ep", "tp", None), P(), P(("ep", "tp"), None),
            P(("ep", "tp"), None), P(("ep", "tp"), None),
        ),
        out_specs=P("ep", "tp"),
        check_vma=False,
    )
```

```python
import jax
import jax.numpy as jnp
from jax import lax
from jax.experimental import pallas as pl
from jax.experimental.pallas import tpu as pltpu
from jax.sharding import PartitionSpec as P


HEAD = 64
CACHE = 1024
WIDTH = 2048
ROWS = 16
LANES = 128
HALF = 8
KIB = 1024
MESSAGES = 768
PART = 256
EACH = 24
RETURNED = 512
epsilon = 1e-06
NT = (((1,), (1,)), ((), ()))
VMEM = pl.BlockSpec(memory_space=pltpu.VMEM)
SMEM = pl.BlockSpec(memory_space=pltpu.SMEM)
HBM = pl.BlockSpec(memory_space=pltpu.HBM)


def columns_of(pair):
    r = lax.broadcasted_iota(jnp.int32, (ROWS, ROWS), 0)
    c = lax.broadcasted_iota(jnp.int32, (ROWS, ROWS), 1)
    pair = pair.astype(jnp.float32)
    return [
        jnp.sum(jnp.where(r == c, pair[k : k + 1], 0.0), axis=-1, keepdims=True) for k in range(2)
    ]


def hits_of(routes, expert, slot):
    first, second = [expert == c.astype(jnp.int32) for c in columns_of(routes)]
    hit = (first | second).astype(jnp.float32).astype(jnp.bfloat16)
    r = lax.broadcasted_iota(jnp.int32, (ROWS, ROWS), 0)
    c = lax.broadcasted_iota(jnp.int32, (ROWS, ROWS), 1)
    before = jnp.dot(
        (c < r).astype(jnp.float32).astype(jnp.bfloat16), hit, preferred_element_type=jnp.float32
    )
    right = before == slot.astype(jnp.float32)
    return first & right, second & right


def quarter_of(device):
    return 4 * (2 * ((device >> 2) & 1) + (device & 1))


def picks_of(routes):
    shape = (ROWS, MESSAGES)
    row = lax.broadcasted_iota(jnp.int32, shape, 0)
    col = lax.broadcasted_iota(jnp.int32, shape, 1)
    block = jnp.zeros(shape, jnp.int32)
    for k in range(1, 32):
        block = block + (col >= k * EACH).astype(jnp.int32)
    inner = col - block * EACH
    q = jnp.zeros(shape, jnp.int32)
    for k in range(1, 4):
        q = q + (inner >= k * 6).astype(jnp.int32)
    place, device = inner - 6 * q, 31 - block
    first, second = hits_of(routes, device, place)
    expert = (first | second) & (place < 2)
    dense = (row == quarter_of(device) + place - 2) & (place >= 2)
    pick = jnp.where(expert | dense, 1.0, 0.0)
    stacked = jnp.concatenate([jnp.where(q == k, pick, 0.0) for k in range(4)], axis=0)
    return stacked.astype(jnp.bfloat16)


def attention_kernel(
    len_hbm, bias_hbm, tok_hbm, gain_hbm, hgain_hbm, route_hbm, wq_hbm, kv_hbm, wo_hbm,
    out_ref, pick_ref,
    len_v, bias_v, tok_v, gain_v, hgain_v, route_v,
    wq_v, kv_v, key_v, value_v, wo_v, small_sem, q_sem, kv_sem, o_sem,
):
    smalls = [
        pltpu.make_async_copy(src, dst, small_sem.at[k])
        for k, (src, dst) in enumerate((
            (tok_hbm, tok_v), (gain_hbm, gain_v), (route_hbm, route_v), (len_hbm, len_v),
            (bias_hbm, bias_v), (hgain_hbm, hgain_v),
        ))
    ]
    for copy in smalls:
        copy.start()
    copy_q = pltpu.make_async_copy(wq_hbm, wq_v, q_sem)
    copy_q.start()
    copies = []
    for s in range(ROWS):
        copy = pltpu.make_async_copy(kv_hbm.at[s, 0], kv_v.at[s], kv_sem.at[s])
        copy.start()
        copies.append(copy)
    copy_o = pltpu.make_async_copy(wo_hbm, wo_v, o_sem)
    copy_o.start()
    for copy in smalls:
        copy.wait()
    wide = tok_v[...].astype(jnp.float32)
    scale = lax.rsqrt(jnp.mean(wide * wide, axis=-1, keepdims=True) + epsilon)
    normed = (wide * scale * gain_v[...]).astype(jnp.bfloat16)
    normed = jnp.concatenate([normed[:, : WIDTH // 2], normed[:, WIDTH // 2 :]], axis=0)
    pick_ref[...] = picks_of(route_v[...])

    lane = lax.broadcasted_iota(jnp.int32, (HALF, LANES), 1)
    row = lax.broadcasted_iota(jnp.int32, (HALF, LANES), 0)
    tri_row = lax.broadcasted_iota(jnp.int32, (LANES, 2 * LANES), 0)
    tri_col = lax.broadcasted_iota(jnp.int32, (LANES, 2 * LANES), 1)
    tri = ((tri_row >= tri_col) | (tri_col >= LANES)).astype(jnp.bfloat16)
    position = lax.broadcasted_iota(jnp.int32, (HALF, CACHE), 1)
    bias = jnp.where(row[:, :1] < 4, bias_v[:, 0:1], bias_v[:, 1:2])
    lengths = len_v[...].astype(jnp.float32)
    seq = lax.broadcasted_iota(jnp.int32, (HALF, ROWS), 1)
    seq_row = lax.broadcasted_iota(jnp.int32, (HALF, ROWS), 0) % 4
    wide_lane = lax.broadcasted_iota(jnp.int32, (CACHE, LANES), 1)
    chunks = CACHE // LANES

    copy_q.wait()
    folded = jnp.concatenate([wq_v[: WIDTH // 2], wq_v[WIDTH // 2 :]], axis=1)
    query = jnp.dot(normed, folded, preferred_element_type=jnp.float32)
    query = query[:ROWS, :LANES] + query[ROWS:, LANES:]
    query = query.astype(jnp.bfloat16).astype(jnp.float32)

    def scored(group):
        part = query[group // 2 * HALF : group // 2 * HALF + HALF]
        swapped = pltpu.roll(part, 4, 0)
        upper, under = (swapped, part) if group % 2 else (part, swapped)
        part = jnp.where(row < 4, upper, under)
        turned = pltpu.roll(part, HEAD, 1)
        first, second = jnp.where(row < 4, part, turned), jnp.where(row < 4, turned, part)
        blocks = []
        for p in range(2):
            low = (row % 4 == 2 * p) & (lane < HEAD)
            high = (row % 4 == 2 * p + 1) & (lane >= HEAD)
            blocks.append(jnp.where(low, first, jnp.where(high, second, 0.0)))
            j = group * 4 + 2 * p
            copies[j].wait()
            copies[j + 1].wait()
            even = kv_v[j]
            odd = pltpu.roll(kv_v[j + 1].astype(jnp.float32), HEAD, 1).astype(jnp.bfloat16)
            key_v[group, :, p * LANES : (p + 1) * LANES] = jnp.where(wide_lane < HEAD, even, odd)
            value_v[group, :, p * LANES : (p + 1) * LANES] = jnp.where(wide_lane < HEAD, odd, even)
        lhs = jnp.concatenate(blocks, axis=1).astype(jnp.bfloat16)
        scores = lax.dot_general(lhs, key_v[group], NT, preferred_element_type=jnp.float32)
        return scores * 0.125 + bias

    def attended(group, scores):
        mine = jnp.where(seq == group * 4 + seq_row, lengths, 0.0)
        valid = position < jnp.sum(mine, axis=-1, keepdims=True).astype(jnp.int32)
        soft = jnp.maximum(scores, 0.0) + jnp.log1p(jnp.exp(-jnp.abs(scores)))
        soft = jnp.where(valid, soft, 0.0)
        stacked = jnp.concatenate(
            [soft[:, c * LANES : (c + 1) * LANES] for c in range(chunks)], axis=0
        )
        high = stacked.astype(jnp.bfloat16)
        rest = stacked - high.astype(jnp.float32)
        middle = rest.astype(jnp.bfloat16)
        low = (rest - middle.astype(jnp.float32)).astype(jnp.bfloat16)
        sums = jnp.dot(
            jnp.concatenate([high, middle, low], axis=0), tri, preferred_element_type=jnp.float32
        )
        size = chunks * HALF
        sums = sums[:size] + sums[size : 2 * size] + sums[2 * size :]
        pieces = [None] * chunks
        carry = jnp.zeros((HALF, LANES), jnp.float32)
        for c in reversed(range(chunks)):
            rows = sums[c * HALF : (c + 1) * HALF]
            pieces[c] = rows[:, :LANES] + carry
            carry = carry + rows[:, LANES:]
        later = jnp.concatenate(pieces, axis=1)
        weights = jnp.where(valid, jnp.exp(scores - later), 0.0).astype(jnp.bfloat16)
        mixed = jnp.dot(weights, value_v[group], preferred_element_type=jnp.float32)
        own = jnp.zeros((HALF, LANES), jnp.float32)
        for p in range(2):
            here = (row % 4 == 2 * p) & (lane >= HEAD)
            here = here | ((row % 4 == 2 * p + 1) & (lane < HEAD))
            own = jnp.where(here, mixed[:, p * LANES : (p + 1) * LANES], own)
        mean = jnp.sum(own * own, axis=-1, keepdims=True) * (1.0 / HEAD)
        own = (own + pltpu.roll(own, HEAD, 1)) * lax.rsqrt(mean + epsilon)
        return jnp.where(lane < HEAD, own, pltpu.roll(own, 4, 0)) * hgain_v[...]

    scores = scored(0)
    heads = []
    for group in range(4):
        later_scores = scored(group + 1) if group < 3 else None
        heads.append(attended(group, scores))
        scores = later_scores
    head_rows = jnp.concatenate(
        [jnp.where(row < 4, heads[2 * k], pltpu.roll(heads[2 * k + 1], 4, 0)) for k in range(2)],
        axis=0,
    ).astype(jnp.bfloat16)
    copy_o.wait()
    share = jnp.dot(head_rows, wo_v[...], preferred_element_type=jnp.float32)
    out_ref[...] = share.astype(jnp.bfloat16)


def in_hbm(*arrays):
    return [pltpu.with_memory_space_constraint(a, pltpu.HBM) for a in arrays]


def attention(
    tokens, attn_gain, w_query, stick_bias, kv_cache, lengths, head_gain, w_attn_out, routes
):
    return pl.pallas_call(
        attention_kernel,
        out_shape=(
            pltpu.VMEM((ROWS, WIDTH), jnp.bfloat16),
            pltpu.VMEM((4 * ROWS, MESSAGES), jnp.bfloat16),
        ),
        in_specs=[HBM] * 9,
        out_specs=(VMEM, VMEM),
        scratch_shapes=[
            pltpu.VMEM((1, ROWS), jnp.int32),
            pltpu.VMEM((1, 2), jnp.float32),
            pltpu.VMEM((ROWS, WIDTH), jnp.bfloat16),
            pltpu.VMEM((1, WIDTH), jnp.float32),
            pltpu.VMEM((1, LANES), jnp.float32),
            pltpu.VMEM((2, ROWS), jnp.int32),
            pltpu.VMEM((WIDTH, LANES), jnp.bfloat16),
            pltpu.VMEM((ROWS, CACHE, LANES), jnp.bfloat16),
            pltpu.VMEM((4, CACHE, 2 * LANES), jnp.bfloat16),
            pltpu.VMEM((4, CACHE, 2 * LANES), jnp.bfloat16),
            pltpu.VMEM((LANES, WIDTH), jnp.bfloat16),
            pltpu.SemaphoreType.DMA((6,)),
            pltpu.SemaphoreType.DMA,
            pltpu.SemaphoreType.DMA((ROWS,)),
            pltpu.SemaphoreType.DMA,
        ],
        cost_estimate=pl.CostEstimate(
            flops=400_000_000, bytes_accessed=6_000_000, transcendentals=200_000
        ),
    )(
        *in_hbm(
            lengths.reshape(1, -1), stick_bias.reshape(1, -1), tokens, attn_gain.reshape(1, -1),
            head_gain.reshape(1, -1), routes.T, w_query, kv_cache, w_attn_out,
        ),
    )


def mix_kernel(route_ref, weight_ref, branch_ref, mix_ref):
    shape = (ROWS, RETURNED)
    row = lax.broadcasted_iota(jnp.int32, shape, 0)
    col = lax.broadcasted_iota(jnp.int32, shape, 1)
    device, place, side = 31 - (col >> 4), (col >> 1) & 7, col & 1
    first, second = hits_of(route_ref[...], device, place)
    one, two = columns_of(weight_ref[...])
    expert = jnp.where(first, one, jnp.where(second, two, 0.0))
    here = (row == quarter_of(device) + place - 2) & (place < 6)
    dense = jnp.where(here, branch_ref[:, 0:1], 0.0)
    value = jnp.where(place < 2, expert, dense)
    both = jnp.concatenate([jnp.where(side == h, value, 0.0) for h in range(2)], axis=0)
    mix_ref[...] = both.astype(jnp.bfloat16)


def mix_table(routes, weights, branch):
    return pl.pallas_call(
        mix_kernel,
        out_shape=jax.ShapeDtypeStruct((2 * ROWS, RETURNED), jnp.bfloat16),
        in_specs=[VMEM, VMEM, VMEM],
        out_specs=VMEM,
        compiler_params=pltpu.CompilerParams(vmem_limit_bytes=8192 * KIB),
        cost_estimate=pl.CostEstimate(
            flops=1_000_000, bytes_accessed=100_000, transcendentals=0
        ),
    )(routes.T, weights.T, branch)


def dispatch_kernel(
    a_ref, b_ref, c_ref, d_ref, tok_ref, gain_ref, gate_ref, pick_ref,
    send_ref, res_ref, branch_ref, total_v,
):
    total = a_ref[...].astype(jnp.float32) + b_ref[...].astype(jnp.float32)
    total = total + (c_ref[...].astype(jnp.float32) + d_ref[...].astype(jnp.float32))
    total = total + tok_ref[...].astype(jnp.float32)
    total_v[...] = total
    at = pl.multiple_of(lax.axis_index("tp") * 256, 256)
    res_ref[...] = total_v[:, pl.ds(at, 256)]
    scale = lax.rsqrt(jnp.mean(total * total, axis=-1, keepdims=True) + epsilon)
    normed = (total * scale * gain_ref[...]).astype(jnp.bfloat16)
    logit = jnp.sum(
        normed.astype(jnp.float32) * gate_ref[...].astype(jnp.float32), axis=-1, keepdims=True
    )
    branch_ref[...] = jnp.broadcast_to(1.0 / (1.0 + jnp.exp(-logit)), branch_ref.shape)
    lower = lax.axis_index("tp") % 2 == 0
    normed = jnp.where(
        lower, normed[:, : WIDTH // 2].astype(jnp.float32), normed[:, WIDTH // 2 :].astype(jnp.float32)
    ).astype(jnp.bfloat16)
    stacked = jnp.concatenate([normed[:, q * PART : (q + 1) * PART] for q in range(4)], axis=0)
    send_ref[...] = lax.dot_general(
        pick_ref[...], stacked, (((0,), (0,)), ((), ())), preferred_element_type=jnp.float32
    ).astype(jnp.bfloat16)


def dispatch(shares, tokens, ffn_gain, branch_gate, picks):
    return pl.pallas_call(
        dispatch_kernel,
        out_shape=(
            jax.ShapeDtypeStruct((MESSAGES, PART), jnp.bfloat16),
            jax.ShapeDtypeStruct((ROWS, 256), jnp.float32),
            jax.ShapeDtypeStruct((ROWS, LANES), jnp.float32),
        ),
        in_specs=[VMEM] * 8,
        out_specs=(VMEM, VMEM, VMEM),
        scratch_shapes=[pltpu.VMEM((ROWS, WIDTH), jnp.float32)],
        compiler_params=pltpu.CompilerParams(vmem_limit_bytes=8192 * KIB),
        cost_estimate=pl.CostEstimate(
            flops=40_000_000, bytes_accessed=1_500_000, transcendentals=100
        ),
    )(*shares, tokens, ffn_gain.reshape(1, -1), branch_gate.reshape(1, -1), picks)


def warm_kernel(gate_hbm, up_hbm, down_hbm, gate_out, up_out, down_out, sems):
    copies = [
        pltpu.make_async_copy(gate_hbm, gate_out, sems.at[0]),
        pltpu.make_async_copy(up_hbm, up_out, sems.at[1]),
        pltpu.make_async_copy(down_hbm, down_out, sems.at[2]),
    ]
    for copy in copies:
        copy.start()
    for copy in copies:
        copy.wait()


def warm(gate, up, down):
    return pl.pallas_call(
        warm_kernel,
        out_shape=(pltpu.VMEM((WIDTH, 256), jnp.bfloat16),) * 2
        + (pltpu.VMEM((256, WIDTH), jnp.bfloat16),),
        in_specs=[HBM] * 3,
        out_specs=(VMEM,) * 3,
        scratch_shapes=[pltpu.SemaphoreType.DMA((3,))],
        compiler_params=pltpu.CompilerParams(vmem_limit_bytes=4096 * KIB),
        cost_estimate=pl.CostEstimate(
            flops=1_000_000, bytes_accessed=4_000_000, transcendentals=0
        ),
    )(*in_hbm(gate, up, down))


def feed_kernel(got_ref, other_ref, eg_ref, eu_ref, ed_ref, *rest):
    packs = rest[:4]
    keep_ref, send_ref, wide_v, both_v, dd_v, d_sem = rest[4:]
    lower = lax.axis_index("tp") % 2 == 0
    targets = ((both_v, 0), (both_v, 128), (dd_v, 0))
    dense_copies = [
        pltpu.make_async_copy(
            pack.at[k], dst.at[pl.ds(at + 32 * i, 32), :], d_sem.at[4 * k + i]
        )
        for k, (dst, at) in enumerate(targets)
        for i, pack in enumerate(packs)
    ]
    for copy in dense_copies:
        copy.start()
    for l in range(2):
        mine = got_ref[:, l * LANES : (l + 1) * LANES].astype(jnp.float32)
        theirs = other_ref[:, l * LANES : (l + 1) * LANES].astype(jnp.float32)
        wide_v[l] = jnp.where(lower, mine, theirs)
        wide_v[2 + l] = jnp.where(lower, theirs, mine)

    def unpacked(places):
        parts = [
            jnp.concatenate(
                [wide_v[2 * s + l, pl.ds(q * 6 + j, 32, stride=EACH), :] for j in places], axis=0
            )
            for s in range(2)
            for q in range(4)
            for l in range(2)
        ]
        return jnp.concatenate(parts, axis=1).astype(jnp.bfloat16)

    def packed(first, value):
        here = slice(first, first + value.shape[0])
        for y in range(4):
            even = value[:, 512 * y : 512 * y + 256]
            odd = value[:, 512 * y + 256 : 512 * y + 512]
            there = slice(256 * y, 256 * y + 256)
            keep_ref[here, there] = jnp.where(lower, even, odd)
            send_ref[here, there] = jnp.where(lower, odd, even).astype(jnp.bfloat16)

    rows = unpacked((0, 1))
    dense_rows = unpacked((2, 3, 4, 5))
    a = jnp.dot(rows, eg_ref[...], preferred_element_type=jnp.float32)
    b = jnp.dot(rows, eu_ref[...], preferred_element_type=jnp.float32)
    hidden = (a / (1.0 + jnp.exp(-a)) * b).astype(jnp.bfloat16)
    packed(0, jnp.dot(hidden, ed_ref[...], preferred_element_type=jnp.float32))
    for copy in dense_copies[:8]:
        copy.wait()
    both = lax.dot_general(dense_rows, both_v[...], NT, preferred_element_type=jnp.float32)
    a, b = both[:, :128], both[:, 128:]
    hidden = (a / (1.0 + jnp.exp(-a)) * b).astype(jnp.bfloat16)
    for copy in dense_copies[8:]:
        copy.wait()
    packed(64, jnp.dot(hidden, dd_v[...], preferred_element_type=jnp.float32))


def feed(got, other, gate, up, down, packs):
    return pl.pallas_call(
        feed_kernel,
        out_shape=(
            jax.ShapeDtypeStruct((192, 1024), jnp.float32),
            jax.ShapeDtypeStruct((192, 1024), jnp.bfloat16),
        ),
        in_specs=[VMEM] * 5 + [HBM] * 4,
        out_specs=(VMEM, VMEM),
        scratch_shapes=[
            pltpu.VMEM((4, MESSAGES, LANES), jnp.float32),
            pltpu.VMEM((256, WIDTH), jnp.bfloat16),
            pltpu.VMEM((128, WIDTH), jnp.bfloat16),
            pltpu.SemaphoreType.DMA((12,)),
        ],
        compiler_params=pltpu.CompilerParams(vmem_limit_bytes=24576 * KIB),
        cost_estimate=pl.CostEstimate(
            flops=1_000_000_000, bytes_accessed=7_000_000, transcendentals=40_000
        ),
    )(got, other, gate, up, down, *packs)


def halve_kernel(keep_ref, got_ref, out_ref, one_ref, two_ref, three_ref, sum_v):
    y = lax.axis_index("tp") // 2
    for k in range(4):
        there = slice(256 * k, 256 * k + 256)
        sum_v[k] = keep_ref[:, there] + got_ref[:, there].astype(jnp.float32)
    out_ref[...] = sum_v[y]
    for step, ref in ((1, one_ref), (2, two_ref), (3, three_ref)):
        ref[...] = sum_v[(y + step) % 4].astype(jnp.bfloat16)


def halve(keep, got):
    return pl.pallas_call(
        halve_kernel,
        out_shape=(jax.ShapeDtypeStruct((192, 256), jnp.float32),)
        + (jax.ShapeDtypeStruct((192, 256), jnp.bfloat16),) * 3,
        in_specs=[VMEM] * 2,
        out_specs=(VMEM,) * 4,
        scratch_shapes=[pltpu.VMEM((4, 192, 256), jnp.float32)],
        compiler_params=pltpu.CompilerParams(vmem_limit_bytes=8192 * KIB),
        cost_estimate=pl.CostEstimate(
            flops=1_000_000, bytes_accessed=1_000_000, transcendentals=0
        ),
    )(keep, got)


def pack_kernel(a_ref, b_ref, c_ref, d_ref, out_ref, back_v):
    total = a_ref[...] + b_ref[...].astype(jnp.float32)
    total = total + (c_ref[...].astype(jnp.float32) + d_ref[...].astype(jnp.float32))
    for place in range(8):
        for h in range(2):
            if place < 6:
                piece = total[place * 32 : place * 32 + 32, h * LANES : (h + 1) * LANES]
            else:
                piece = jnp.zeros((32, LANES), jnp.float32)
            back_v[pl.ds(place * 2 + h, 32, stride=16), :] = piece
    out_ref[...] = back_v[...].astype(jnp.bfloat16)


def pack(blocks):
    return pl.pallas_call(
        pack_kernel,
        out_shape=jax.ShapeDtypeStruct((RETURNED, LANES), jnp.bfloat16),
        in_specs=[VMEM] * 4,
        out_specs=VMEM,
        scratch_shapes=[pltpu.VMEM((RETURNED, LANES), jnp.float32)],
        compiler_params=pltpu.CompilerParams(vmem_limit_bytes=8192 * KIB),
        cost_estimate=pl.CostEstimate(
            flops=1_000_000, bytes_accessed=500_000, transcendentals=0
        ),
    )(*blocks)


def finish_kernel(mix_ref, got_ref, res_ref, out_ref):
    total = jnp.dot(mix_ref[...], got_ref[...], preferred_element_type=jnp.float32)
    total = jnp.concatenate([total[:ROWS], total[ROWS:]], axis=1)
    out_ref[...] = (res_ref[...] + total).astype(jnp.bfloat16)


def finish(mix, returned, residual):
    return pl.pallas_call(
        finish_kernel,
        out_shape=jax.ShapeDtypeStruct((ROWS, 256), jnp.bfloat16),
        in_specs=[VMEM] * 3,
        out_specs=VMEM,
        compiler_params=pltpu.CompilerParams(vmem_limit_bytes=8192 * KIB),
        cost_estimate=pl.CostEstimate(
            flops=40_000_000, bytes_accessed=600_000, transcendentals=0
        ),
    )(mix, returned, residual)


def along_y(x, step):
    return lax.ppermute(x, "tp", [(i, (i + 2 * step) % 8) for i in range(8)])


def layer(
    tokens, attn_gain, w_query, stick_bias, kv_cache, lengths, head_gain, w_attn_out, ffn_gain,
    route_expert, route_weight, w_exp_gate, w_exp_up, w_exp_down, branch_gate,
    w_dense_gate, w_dense_up, w_dense_down,
):
    single, half = jnp.float32, jnp.bfloat16
    swap = [(i, i ^ 1) for i in range(8)]

    square = [(i, i ^ 1) for i in range(32)]
    own = lax.optimization_barrier(jnp.stack([w_dense_gate, w_dense_up, w_dense_down]))
    packs = [own, lax.ppermute(own, "ep", [(i, i ^ 4) for i in range(32)])]
    packs.append(lax.ppermute(own, "ep", square))
    share, picks = attention(
        tokens, attn_gain, w_query, stick_bias, kv_cache, lengths, head_gain, w_attn_out,
        route_expert,
    )
    other = lax.ppermute(share, "tp", swap)
    share = (share.astype(single) + other.astype(single)).astype(half)
    shares = [share]
    for step in (1, 3, 2):
        shares.append(along_y(share, step))
    packs.append(lax.ppermute(packs[1], "ep", square))
    send, residual, branch = dispatch(shares, tokens, ffn_gain, branch_gate, picks)
    got = lax.all_to_all(
        send.reshape(32, EACH, PART), "ep", 0, 0, tiled=True,
        axis_index_groups=[list(range(31, -1, -1))],
    )

    mix = mix_table(route_expert, route_weight, branch)
    gate, up, down = warm(w_exp_gate[0], w_exp_up[0], w_exp_down[0])
    got = got.reshape(MESSAGES, PART)
    other = lax.ppermute(got, "tp", swap)
    keep, give = feed(got, other, gate, up, down, packs)
    taken = lax.ppermute(give, "tp", swap)
    mine, *others = halve(keep, taken)
    blocks = [mine]
    for step in (1, 3, 2):
        blocks.append(along_y(others[step - 1], step))
    back = pack(blocks)
    returned = lax.all_to_all(
        back.reshape(32, 16, LANES), "ep", 0, 0, tiled=True,
        axis_index_groups=[list(range(31, -1, -1))],
    )
    return finish(mix, returned.reshape(RETURNED, LANES), residual)


def solution(mesh):
    return jax.shard_map(
        layer,
        mesh=mesh,
        in_specs=(
            P("ep", None), P(), P(None, "tp"), P("tp"), P("ep", "tp", None, None), P("ep"),
            P("tp"), P("tp", None), P(), P("ep", None), P("ep", None), P("ep", None, "tp"),
            P("ep", None, "tp"), P("ep", "tp", None), P(), P(("ep", "tp"), None),
            P(("ep", "tp"), None), P(("ep", "tp"), None),
        ),
        out_specs=P("ep", "tp"),
        check_vma=False,
    )
```
